32 devices in a mesh: sp: 16 (over z, y, x), tp: 2 (over core).
Axes of the slice: x: 2, y: 2, z: 4, core: 2. Of those that a mesh axis runs over, the one named last changes fastest.
Arguments:
- residual: bfloat16 [4096, 2048], P(('sp', 'tp')), may hold values from -6 to 6
- queries: bfloat16 [4096, 512], P('sp', 'tp'), may hold values from -6 to 6
- key_rows: bfloat16 [4096, 512], P('sp', 'tp'), may hold values from -6 to 6
- value_rows: bfloat16 [4096, 1024], P('sp', 'tp'), may hold values from -6 to 6
- out_gate: bfloat16 [4096, 1024], P('sp', 'tp'), may hold values from -6 to 6
- gate_logits: bfloat16 [4096, 512], P('sp', 'tp')
- head_gain: float32 [128], replicated, may hold values from 0.1 to 1.9
- out_weight: bfloat16 [1024, 2048], replicated, may hold values from -0.1875 to 0.1875
- norm_gain: float32 [2048], replicated, may hold values from 0.1 to 1.9
- routes: int32 [4096, 2], P(('sp', 'tp')), may hold values from 0 to 31, as said below
- group_score: float32 [4096], P(('sp', 'tp')), may hold values from 0.25 to 1
- expert_score: float32 [4096, 2], P(('sp', 'tp')), may hold values from 0.1 to 1
- gate_weight: bfloat16 [32, 2048, 512], P(('sp', 'tp')), may hold values from -0.125 to 0.125
- up_weight: bfloat16 [32, 2048, 512], P(('sp', 'tp')), may hold values from -0.125 to 0.125
- down_weight: bfloat16 [32, 512, 2048], P(('sp', 'tp')), may hold values from -0.25 to 0.25
Outputs:
- layer_out: bfloat16 [4096, 2048], P(('sp', 'tp'))
The draws below stay inside these ranges and needn't reach their ends.
Inputs may be any that keep to these rules, and one draw needn't show every extreme that they name: `routes`: the two experts of a token differ and lie in one group of 8 consecutive expert numbers. In each aligned block of 128 tokens (the tokens of one device) no expert is named more than 12 times, and one expert, the same for all blocks of a draw, is named exactly 12 times in every block.
All inputs are finite; a program needn't handle non-finite values.
Results may differ from the reference program's by a relative error of at most 0.0056.
Values may be sent and summed in bfloat16 or wider, within the bound.
A program may use at most 64 MiB of HBM per device.

```python
import math
from functools import partial
import jax
import jax.numpy as jnp
from jax import lax

MODEL_WIDTH = 2048
HEADS = 8
KEY_DIM = 64
VALUE_DIM = 128
EXPERT_WIDTH = 512
GROUP_SIZE = 8
BLOCK = 64
SEGMENT = 256
KEYS = 512
VALUES = 1024
ROWS = 128
TOKENS = 4096
EXPERTS = 32
GROUPS = 4
CAPACITY = 12


def draw_gate_logits(key, part):
    subkeys = jax.random.split(key, 7)
    slow_share = 0.5
    slow_heads = jax.random.bernoulli(subkeys[0], slow_share, (HEADS,))
    chain_loss = jnp.exp(jax.random.uniform(subkeys[1], (HEADS, KEY_DIM), jnp.float32, jnp.log(0.2), jnp.log(0.8)))
    slow_logit = jnp.log(TOKENS / (16.0 * chain_loss))
    fast_rate = jnp.exp(jax.random.uniform(subkeys[2], (HEADS, KEY_DIM), jnp.float32, jnp.log(1.0 / 100.0), jnp.log(1.0 / 30.0)))
    fast_logit = -jnp.log(jnp.expm1(16.0 * fast_rate))
    base_logit = jnp.where(slow_heads[:, None], slow_logit, fast_logit)
    jitter = jax.random.uniform(subkeys[3], (TOKENS, HEADS, KEY_DIM), jnp.float32, -1.0, 1.0)
    offset = jax.random.uniform(subkeys[4], (TOKENS // SEGMENT, HEADS), jnp.float32, -0.7, 0.7)
    offset = jnp.repeat(offset, SEGMENT, axis=0)
    router_scores = base_logit[None] + jitter + offset[:, :, None]
    slot_places = jax.random.randint(subkeys[5], (2, HEADS), 0, TOKENS)
    spike_strength = jax.random.uniform(subkeys[6], (2, HEADS), jnp.float32, -11.0, -4.0)
    token_position = jnp.arange(TOKENS, dtype=jnp.int32)[:, None]
    spike_value = jnp.where(token_position == slot_places[0][None, :], spike_strength[0][None, :], spike_strength[1][None, :])
    spike_mask = (token_position == slot_places[0][None, :]) | (token_position == slot_places[1][None, :])
    router_scores = jnp.where(spike_mask[:, :, None], spike_value[:, :, None], router_scores)
    return router_scores.reshape(TOKENS, HEADS * KEY_DIM).astype(jnp.bfloat16)


def shuffle_group(group_key):
    return jax.random.permutation(group_key, GROUP_SIZE).astype(jnp.int32)


def route_block(block_key, hot_expert):
    subkeys = jax.random.split(block_key, 4)
    slot_total = GROUPS * 3 * CAPACITY
    labels = (jax.random.permutation(subkeys[0], slot_total) // (3 * CAPACITY)).astype(jnp.int32)
    chosen = labels[:5 * ROWS // 8]
    group_index = jnp.arange(GROUPS, dtype=jnp.int32)
    extra_count = jnp.sum((chosen[:, None] == group_index[None, :]).astype(jnp.int32), axis=0)
    tickets = 2 * CAPACITY + 2 * extra_count
    group_rows = tickets // 2
    hot_group = hot_expert // GROUP_SIZE
    hot_local = hot_expert % GROUP_SIZE
    orders = jax.vmap(shuffle_group)(jax.random.split(subkeys[1], GROUPS))
    rank_grid = jnp.arange(GROUP_SIZE, dtype=jnp.int32)[None, :]
    hot_row = (group_index == hot_group)[:, None]
    sort_key = jnp.where(hot_row & (orders == hot_local), -1, rank_grid)
    orders = jnp.take_along_axis(orders, jnp.argsort(sort_key, axis=1, stable=True), axis=1)
    remaining = tickets[:, None] - CAPACITY
    hot_counts = jnp.where(rank_grid == 0, CAPACITY, remaining // (GROUP_SIZE - 1) + (rank_grid - 1 < remaining % (GROUP_SIZE - 1)).astype(jnp.int32))
    drawn_counts = tickets[:, None] // GROUP_SIZE + (rank_grid < tickets[:, None] % GROUP_SIZE).astype(jnp.int32)
    counts = jnp.where(hot_row, hot_counts, drawn_counts)
    count_ends = jnp.cumsum(counts, axis=1)
    row_ends = jnp.cumsum(group_rows)
    row_ids = jnp.arange(ROWS, dtype=jnp.int32)
    group_of = jnp.sum((row_ids[:, None] >= row_ends[None, :]).astype(jnp.int32), axis=1)
    start_of = row_ends[group_of] - group_rows[group_of]
    first_pos = row_ids - start_of
    second_pos = first_pos + group_rows[group_of]
    ends_table = count_ends[group_of]
    first_rank = jnp.sum((first_pos[:, None] >= ends_table).astype(jnp.int32), axis=1)
    second_rank = jnp.sum((second_pos[:, None] >= ends_table).astype(jnp.int32), axis=1)
    order_rows = orders[group_of]
    first_expert = group_of * GROUP_SIZE + jnp.take_along_axis(order_rows, first_rank[:, None], axis=1)[:, 0]
    second_expert = group_of * GROUP_SIZE + jnp.take_along_axis(order_rows, second_rank[:, None], axis=1)[:, 0]
    expert_pairs = jnp.stack([first_expert, second_expert], axis=1)
    flip_order = jax.random.randint(subkeys[2], (ROWS,), 0, 2)
    expert_pairs = jnp.where(flip_order[:, None] == 1, expert_pairs[:, ::-1], expert_pairs)
    shuffled = expert_pairs[jax.random.permutation(subkeys[3], ROWS)]
    return shuffled.astype(jnp.int32)


def draw_routes(key, part):
    hot_expert = jax.random.randint(jax.random.fold_in(key, 11), (), 0, EXPERTS)
    block_keys = jax.random.split(jax.random.fold_in(key, 12), TOKENS // ROWS)
    blocks_out = jax.vmap(partial(route_block, hot_expert=hot_expert))(block_keys)
    return blocks_out.reshape(TOKENS, 2).astype(jnp.int32)


def block_scale(stream_key, dims, cuts, smallest, top_value):
    factor_of = 1.0
    for position, blocks in cuts:
        steps = jax.random.uniform(jax.random.fold_in(jax.random.fold_in(stream_key, 6), position), (blocks,), jnp.float32, smallest / len(cuts), top_value / len(cuts))
        factor_of = factor_of * jnp.repeat(jnp.exp(steps), dims[position] // blocks).reshape((-1,) + (1,) * (len(dims) - 1 - position))
    return factor_of


def gaussian(key, dims, spread, reach, cuts=(), held_as=jnp.bfloat16):
    drawn = jax.random.normal(key, dims, jnp.float32) * spread
    if len(cuts) > 0:
        drawn = block_scale(key, dims, cuts, -0.22, 0.18) * drawn
    return jnp.clip(drawn, min=-reach, max=reach).astype(held_as)


def setup_inputs(seed: int = 0) -> dict:
    arg_keys = jax.random.split(jax.random.key(seed), 16)
    residual = gaussian(arg_keys[0], (TOKENS, MODEL_WIDTH), 1.0, 6.0, ((0, 32),))
    queries = gaussian(arg_keys[1], (TOKENS, KEYS), 1.0, 6.0, ((0, 16), (1, 2)))
    key_rows = gaussian(arg_keys[2], (TOKENS, KEYS), 1.0, 6.0, ((0, 16), (1, 2)))
    value_rows = gaussian(arg_keys[3], (TOKENS, VALUES), 1.0, 6.0, ((0, 16), (1, 2)))
    out_gate = gaussian(arg_keys[4], (TOKENS, VALUES), 1.0, 6.0, ((0, 16), (1, 2)))
    gate_logits = draw_gate_logits(jax.random.fold_in(arg_keys[15], 71), 0)
    head_gain = jnp.clip(1.0 + 0.18 * jax.random.normal(arg_keys[6], (VALUE_DIM,), jnp.float32), 0.1, 1.9)
    out_weight = gaussian(arg_keys[7], (VALUES, MODEL_WIDTH), VALUES ** -0.5, 0.1875)
    norm_gain = jnp.clip(1.0 + 0.18 * jax.random.normal(arg_keys[8], (MODEL_WIDTH,), jnp.float32), 0.1, 1.9)
    routes = draw_routes(jax.random.fold_in(arg_keys[15], 71), 0)
    group_score = jnp.clip(0.25 + 0.75 * jax.random.uniform(arg_keys[10], (TOKENS,), jnp.float32) ** block_scale(arg_keys[10], (TOKENS,), ((0, 32),), -0.2, 0.2), 0.25, 1.0)
    expert_score = jnp.clip(jnp.exp(math.log(1.0) - 2.3025851 * jax.random.uniform(arg_keys[11], (TOKENS, 2), jnp.float32) ** block_scale(arg_keys[11], (TOKENS, 2), ((0, 32),), -0.2, 0.2)), 0.1, 1.0)
    gate_weight = gaussian(arg_keys[12], (EXPERTS, MODEL_WIDTH, EXPERT_WIDTH), MODEL_WIDTH ** -0.5, 0.125, ((0, 32),))
    up_weight = gaussian(arg_keys[13], (EXPERTS, MODEL_WIDTH, EXPERT_WIDTH), MODEL_WIDTH ** -0.5, 0.125, ((0, 32),))
    down_weight = gaussian(arg_keys[14], (EXPERTS, EXPERT_WIDTH, MODEL_WIDTH), EXPERT_WIDTH ** -0.5, 0.25, ((0, 32),))
    return dict(residual=residual, queries=queries, key_rows=key_rows, value_rows=value_rows, out_gate=out_gate, gate_logits=gate_logits, head_gain=head_gain, out_weight=out_weight, norm_gain=norm_gain, routes=routes, group_score=group_score, expert_score=expert_score, gate_weight=gate_weight, up_weight=up_weight, down_weight=down_weight)


def block_parts(queries, key_rows, value_rows, gate_logits):
    length = queries.shape[0]
    head_count = queries.shape[1] // KEY_DIM
    blocks = length // BLOCK

    def arrange(source, inner_size):
        return source.astype(jnp.float32).reshape(blocks, BLOCK, head_count, inner_size).transpose(0, 2, 1, 3)
    decay_log = jax.nn.log_sigmoid(gate_logits.astype(jnp.float32)) / 16.0
    running = jnp.cumsum(arrange(decay_log, KEY_DIM), axis=2)
    closing = running[:, :, -1:, :]
    query_scaled = arrange(queries, KEY_DIM) * KEY_DIM ** (-0.5) * jnp.exp(running)
    key_float = arrange(key_rows, KEY_DIM)
    key_inverse = key_float * jnp.exp(-running)
    key_closing = key_float * jnp.exp(closing - running)
    value_float = arrange(value_rows, VALUE_DIM)
    causal = jnp.tril(jnp.ones((BLOCK, BLOCK), dtype=bool))
    scores = jnp.where(causal, jnp.einsum('nhcd,nhsd->nhcs', query_scaled, key_inverse, precision=lax.Precision.HIGHEST), 0.0)
    within = jnp.einsum('nhcs,nhsv->nhcv', scores, value_float, precision=lax.Precision.HIGHEST)
    increments = jnp.einsum('nhcd,nhcv->nhdv', key_closing, value_float, precision=lax.Precision.HIGHEST)
    return (query_scaled, within, increments, closing[:, :, 0, :])

def advance(carried, inputs):
    increment, block_log = inputs
    return (jnp.exp(block_log)[..., None] * carried + increment, carried)

def finish(attended, head_gain, out_gate):
    blocks = attended.shape[0]
    head_count = attended.shape[1]
    length = blocks * BLOCK
    ordered = attended.transpose(0, 2, 1, 3).reshape(length, head_count, VALUE_DIM)
    normed = ordered * lax.rsqrt(lax.optimization_barrier(jnp.mean(ordered * ordered, axis=-1, keepdims=True)) + 1e-06) * head_gain
    gating = jax.nn.silu(out_gate.astype(jnp.float32)).reshape(length, head_count, VALUE_DIM)
    return (normed * gating).reshape(length, head_count * VALUE_DIM).astype(jnp.bfloat16)

def route_slots(block_routes, experts_total, capacity):
    row_count = block_routes.shape[0]
    flattened = block_routes.reshape(-1)
    onehot = (flattened[:, None] == jnp.arange(experts_total, dtype=jnp.int32)[None, :]).astype(jnp.int32)
    ranking = lax.optimization_barrier(jnp.sum((jnp.cumsum(onehot, axis=0) - onehot) * onehot, axis=1))
    slot_index = flattened * capacity + ranking
    route_ids = jnp.arange(2 * row_count, dtype=jnp.int32) // 2
    owners = jnp.full((experts_total * capacity,), row_count, jnp.int32).at[slot_index].set(route_ids)
    return (slot_index, owners)

def expert_apply(rows_in, gate_matrix, up_matrix, down_matrix):
    gated = jnp.dot(rows_in, gate_matrix, preferred_element_type=jnp.float32)
    lifted = jnp.dot(rows_in, up_matrix, preferred_element_type=jnp.float32)
    inner_rows = (jax.nn.silu(gated) * lifted).astype(jnp.bfloat16)
    return jnp.dot(inner_rows, down_matrix, preferred_element_type=jnp.float32).astype(jnp.bfloat16)

def reference(residual, queries, key_rows, value_rows, out_gate, gate_logits, head_gain, out_weight, norm_gain, routes, group_score, expert_score, gate_weight, up_weight, down_weight):
    query_scaled, within, increments, block_logs = block_parts(queries, key_rows, value_rows, gate_logits)
    zero_state = jnp.zeros(increments.shape[1:], jnp.float32)
    _, states = lax.scan(advance, zero_state, (increments, block_logs))
    attended = within + jnp.einsum('nhcd,nhdv->nhcv', query_scaled, states, precision=lax.Precision.HIGHEST)
    mixer_out = finish(attended, head_gain, out_gate)
    summed = residual.astype(jnp.float32) + jnp.dot(mixer_out, out_weight, preferred_element_type=jnp.float32)
    merged = summed.astype(jnp.bfloat16)
    widened = lax.optimization_barrier(merged).astype(jnp.float32)
    normed = (widened * lax.rsqrt(lax.optimization_barrier(jnp.mean(widened * widened, axis=-1, keepdims=True)) + 1e-06) * norm_gain).astype(jnp.bfloat16)
    tokens_total = residual.shape[0]
    model_width = residual.shape[1]
    blocks = tokens_total // ROWS
    experts_total = gate_weight.shape[0]
    slot_index, owners = jax.vmap(partial(route_slots, experts_total=experts_total, capacity=CAPACITY))(routes.reshape(blocks, ROWS, 2))
    offsets = (jnp.arange(blocks, dtype=jnp.int32) * ROWS)[:, None]
    sources = jnp.where(owners < ROWS, owners + offsets, tokens_total).astype(jnp.int32)
    padded = jnp.concatenate([normed, jnp.zeros((1, model_width), jnp.bfloat16)], axis=0)
    per_expert = sources.reshape(blocks, experts_total, CAPACITY).transpose(1, 0, 2).reshape(experts_total, blocks * CAPACITY)

    def serve(inputs):
        indices, gate_matrix, up_matrix, down_matrix = inputs
        return expert_apply(padded[indices], gate_matrix, up_matrix, down_matrix)
    results = lax.map(serve, (per_expert, gate_weight, up_weight, down_weight))
    expert_ids = routes.reshape(blocks, 2 * ROWS)
    ranking = slot_index - expert_ids * CAPACITY
    block_base = (jnp.arange(blocks, dtype=jnp.int32) * CAPACITY)[:, None]
    token_position = (expert_ids * (blocks * CAPACITY) + block_base + ranking).astype(jnp.int32)
    picked = results.reshape(-1, model_width)[token_position.reshape(-1)].reshape(tokens_total, 2, model_width)
    weights = group_score[:, None] * expert_score / lax.optimization_barrier(jnp.sum(expert_score, axis=1, keepdims=True))
    combined = weights[:, 0:1] * picked[:, 0].astype(jnp.float32) + weights[:, 1:2] * picked[:, 1].astype(jnp.float32)
    return (widened + combined).astype(jnp.bfloat16)
```

```python
import functools

import jax
import jax.numpy as jnp
from jax import lax
from jax.experimental import pallas as pl
from jax.experimental.pallas import tpu as pltpu
from jax.sharding import PartitionSpec as P

KEY_DIM = 64
VALUE_DIM = 128
BLOCK = 64
GROUP_SIZE = 8
MESH = pl.DeviceIdType.MESH
CHUNKS = 4


def dot(a, b):
    return jnp.dot(a, b, preferred_element_type=jnp.float32)


def silu(v):
    return v / (1.0 + jnp.exp(-v))


def layer_kernel(
    sp, tp, gl_hbm, k_hbm, v_hbm, q_hbm, routes_hbm, gscore_hbm, escore_hbm,
    og_hbm, hgain_hbm, res_hbm, gain_hbm, wo_hbm, wg_hbm, wu_hbm, wd_hbm, out_ref,
    gl_ref, k_ref, v_ref, q_ref, routes_ref, gscore_ref, escore_ref,
    og_ref, hgain_ref, res_ref, gain_ref, wo, wg, wu, wd, mixin, merged, normed, sbuf, rbuf, xsend, xin, ysend, yrecv, zsend, zrecv,
    msend, mrecv, gacc, uacc,
    mix_ref, qlead, within, spack, srecv, gpack, grecv, epack, ent,
    ms1, mr1, ms2, mr2, ms3, mr3, isem, mixsem, msem_s, msem_r, s1, r1, s2, r2, s3, r3, s4, r4,
):
    rows, width = res_ref.shape
    half = v_ref.shape[1]
    experts = sp * tp
    cap = 3 * rows // experts
    quad = GROUP_SIZE // tp
    groups = sp // quad
    trow = rbuf_rows(rows, sp, tp)
    erow = groups * cap
    lanes = rbuf.shape[0]
    chunk = width // CHUNKS
    me_sp = lax.axis_index("sp")
    me_tp = lax.axis_index("tp")
    me_g = me_sp // quad
    me_q = me_sp % quad
    me_l = me_q * tp + me_tp

    pairs = (
        (gl_hbm, gl_ref), (k_hbm, k_ref), (v_hbm, v_ref), (q_hbm, q_ref),
        (routes_hbm, routes_ref), (gscore_hbm, gscore_ref), (escore_hbm, escore_ref),
        (og_hbm, og_ref), (hgain_hbm, hgain_ref), (res_hbm, res_ref), (gain_hbm, gain_ref),
        (wo_hbm, wo), (wg_hbm, wg), (wu_hbm, wu), (wd_hbm, wd),
    )
    loads = [pltpu.make_async_copy(h, v, isem.at[i]) for i, (h, v) in enumerate(pairs)]
    weights = loads[11:]

    def far(d):
        g = lax.rem(me_g + d, groups)
        return g, (g * quad + me_q, me_tp)

    def near(d):
        l = lax.rem(me_l + d, GROUP_SIZE)
        return l, (me_g * quad + l // tp, l % tp)

    barrier = pltpu.get_barrier_semaphore()
    for d in range(1, groups):
        pl.semaphore_signal(barrier, inc=1, device_id=far(d)[1], device_id_type=MESH)
    for d in range(1, GROUP_SIZE):
        pl.semaphore_signal(barrier, inc=1, device_id=near(d)[1], device_id_type=MESH)
    for w in loads:
        w.start()

    def remote(src, dst, ssem, rsem, dev):
        return pltpu.make_async_remote_copy(
            src_ref=src, dst_ref=dst, send_sem=ssem, recv_sem=rsem, device_id=dev,
            device_id_type=MESH,
        )

    length, keys = q_ref.shape
    heads = keys // KEY_DIM
    blocks = length // BLOCK
    part = VALUE_DIM // quad
    loads[0].wait()
    logits = gl_ref[...].astype(jnp.float32)
    logs = (jnp.minimum(logits, 0.0) - jnp.log1p(jnp.exp(-jnp.abs(logits)))) / 16.0
    pos_i = lax.broadcasted_iota(jnp.int32, (length, length), 0)
    pos_j = lax.broadcasted_iota(jnp.int32, (length, length), 1)
    causal = (pos_i // BLOCK == pos_j // BLOCK) & (pos_j <= pos_i)
    running = jnp.dot(
        jnp.where(causal, 1.0, 0.0), logs,
        preferred_element_type=jnp.float32, precision=lax.Precision.HIGHEST,
    )
    split = [slice(n * BLOCK, (n + 1) * BLOCK) for n in range(blocks)]
    closing = [running[(n + 1) * BLOCK - 1 : (n + 1) * BLOCK, :] for n in range(blocks)]
    loads[1].wait()
    key_float = k_ref[...].astype(jnp.float32)
    key_closing = [key_float[s] * jnp.exp(closing[n] - running[s]) for n, s in enumerate(split)]
    key_end = list(key_closing)
    tail = jnp.zeros_like(closing[0])
    for n in range(blocks - 1, -1, -1):
        if n < blocks - 1:
            key_end[n] = key_closing[n] * jnp.exp(tail)
        tail = tail + closing[n]
    key_end = jnp.concatenate(key_end, axis=0).astype(jnp.bfloat16)
    low = lax.broadcasted_iota(jnp.int32, (VALUE_DIM, 2 * KEY_DIM), 1) < KEY_DIM
    bf = jnp.bfloat16
    tile = lax.broadcasted_iota(jnp.int32, (16, keys), 0)

    def as_rows(factor):
        high = factor.astype(bf).astype(jnp.float32)
        return jnp.where(tile == 0, high, jnp.where(tile == 1, factor - high, 0.0)).astype(bf)

    def factor_of(rows16):
        wide = rows16.astype(jnp.float32)
        return wide[0:1] + wide[1:2]

    loads[2].wait()
    for p in range(heads // 2):
        pair = slice(p * 2 * KEY_DIM, (p + 1) * 2 * KEY_DIM)
        both = [
            lax.dot_general(
                v_ref[:, h * VALUE_DIM : (h + 1) * VALUE_DIM], key_end[:, pair],
                (((0,), (0,)), ((), ())), preferred_element_type=jnp.float32,
            )
            for h in (2 * p, 2 * p + 1)
        ]
        end = jnp.where(low, both[0], both[1])
        for j in range(quad):
            spack[j, 0:part, pair] = end[j * part : (j + 1) * part].astype(bf)
    decay_rows = as_rows(jnp.exp(tail))
    for j in range(quad):
        spack[j, part : part + 16, :] = decay_rows
    pl.semaphore_wait(barrier, groups - 1 + GROUP_SIZE - 1)

    def side(d):
        j = lax.rem(me_q + d, quad)
        return j, (me_g * quad + j, me_tp)

    hop1 = []
    for d in range(1, quad):
        j, dev = side(d)
        hop1.append(remote(spack.at[j], srecv.at[me_q], ms1.at[d], mr1.at[d], dev))
        hop1[-1].start()
    srecv[me_q] = spack[me_q]

    loads[3].wait()
    query = q_ref[...].astype(jnp.float32) * KEY_DIM ** (-0.5) * jnp.exp(running)
    key_inverse = (key_float * jnp.exp(-running)).astype(jnp.bfloat16)
    query_bf = query.astype(jnp.bfloat16)
    lead = jnp.zeros_like(closing[0])
    for n, s in enumerate(split):
        qlead[s, :] = (query[s] * jnp.exp(lead)).astype(jnp.bfloat16)
        lead = lead + closing[n]
    older = []
    for n in range(1, blocks):
        pieces = []
        gap = jnp.zeros_like(closing[0])
        for m in range(n - 1, -1, -1):
            pieces.insert(0, key_closing[m] if m == n - 1 else key_closing[m] * jnp.exp(gap))
            gap = gap + closing[m]
        pieces.append(jnp.zeros((length - n * BLOCK, keys), jnp.float32))
        older.append(jnp.concatenate(pieces, axis=0).astype(jnp.bfloat16))
    lane2 = lax.broadcasted_iota(jnp.int32, (length, 2 * KEY_DIM), 1)
    nt = (((1,), (1,)), ((), ()))

    def of_head(x, h):
        keep = lane2[: x.shape[0]] < KEY_DIM if h % 2 == 0 else lane2[: x.shape[0]] >= KEY_DIM
        return jnp.where(keep, x, jnp.zeros_like(x))

    for h in range(heads):
        pair = slice(h // 2 * 2 * KEY_DIM, (h // 2 + 1) * 2 * KEY_DIM)
        mine_q = of_head(query_bf[:, pair], h)
        score = lax.dot_general(
            mine_q, key_inverse[:, pair], nt, preferred_element_type=jnp.float32
        )
        past = [jnp.zeros((BLOCK, length), jnp.float32)]
        for n in range(1, blocks):
            past.append(
                lax.dot_general(
                    mine_q[split[n]], older[n - 1][:, pair], nt,
                    preferred_element_type=jnp.float32,
                )
            )
        score = jnp.where(causal, score, jnp.concatenate(past, axis=0)).astype(jnp.bfloat16)
        hv = slice(h * VALUE_DIM, (h + 1) * VALUE_DIM)
        within[:, hv] = dot(score, v_ref[:, hv])

    for m in hop1:
        m.wait_recv()
    total = jnp.zeros((part, keys), jnp.float32)
    total_decay = jnp.ones((1, keys), jnp.float32)
    before_state, before_decay = [], []
    for j in range(quad):
        before_state.append(total)
        before_decay.append(total_decay)
        step = factor_of(srecv[j, part : part + 16, :])
        total = step * total + srecv[j, 0:part, :].astype(jnp.float32)
        total_decay = total_decay * step
    gpack[0:part, :] = total.astype(bf)
    gpack[part : part + 16, :] = as_rows(total_decay)
    hop2 = []
    for d in range(1, groups):
        g, dev = far(d)
        hop2.append(remote(gpack, grecv.at[me_g], ms2.at[d], mr2.at[d], dev))
        hop2[-1].start()
    grecv[me_g] = gpack[...]

    for w in loads[4:11]:
        w.wait()
    sub = lax.broadcasted_iota(jnp.int32, (rows, rows), 0)
    route_t = routes_ref[...].astype(jnp.float32)
    score_t = escore_ref[...]
    scale_t = gscore_ref[...] * score_t / jnp.sum(score_t, axis=0, keepdims=True)
    columns = jnp.where(sub == 0, route_t[0:1, :], 0.0) + jnp.where(sub == 1, route_t[1:2, :], 0.0)
    columns = columns.T
    ra = columns[:, 0:1].astype(jnp.int32)
    rb = columns[:, 1:2].astype(jnp.int32)
    elane = lax.broadcasted_iota(jnp.int32, (rows, 128), 1)
    row_i = lax.broadcasted_iota(jnp.int32, (rows, rows), 0)
    col_i = lax.broadcasted_iota(jnp.int32, (rows, rows), 1)
    strict = jnp.where(col_i < row_i, 1.0, 0.0).astype(jnp.bfloat16)
    is_a = elane == ra
    is_b = elane == rb
    either = (jnp.where(is_a, 1.0, 0.0) + jnp.where(is_b, 1.0, 0.0)).astype(jnp.bfloat16)
    before = dot(strict, either)
    rank_a = jnp.sum(jnp.where(is_a, before, 0.0), axis=1, keepdims=True)
    rank_b = jnp.sum(jnp.where(is_b, before, 0.0), axis=1, keepdims=True)
    group = ra // GROUP_SIZE
    is_g = elane == group
    before_g = dot(strict, jnp.where(is_g, 1.0, 0.0).astype(jnp.bfloat16))
    rank_g = jnp.sum(jnp.where(is_g, before_g, 0.0), axis=1, keepdims=True).astype(jnp.int32)
    base = me_g * cap + 1
    code_a = ((ra % GROUP_SIZE) * erow + base).astype(jnp.float32) + rank_a
    code_b = ((rb % GROUP_SIZE) * erow + base).astype(jnp.float32) + rank_b
    values = jnp.where(elane == 0, code_a, 0.0) + jnp.where(elane == 1, code_b, 0.0)
    values_t = values.T[0:8, :]
    sub8 = lax.broadcasted_iota(jnp.int32, (8, rows), 0)
    values_t = values_t + jnp.where(sub8 == 2, scale_t[0:1, :], 0.0)
    values_t = values_t + jnp.where(sub8 == 3, scale_t[1:2, :], 0.0)
    slot_lane = lax.broadcasted_iota(jnp.int32, (rows, lanes), 1)
    mine = jnp.where(slot_lane == me_g * trow + rank_g, 1.0, 0.0)
    for g in range(groups):
        msend[g] = jnp.dot(
            values_t, jnp.where(group == g, mine, 0.0),
            preferred_element_type=jnp.float32, precision=lax.Precision.HIGHEST,
        )
    mrecv[me_g] = msend[me_g]
    metas = []
    for d in range(1, groups):
        g, dev = far(d)
        metas.append(remote(msend.at[g], mrecv.at[me_g], msem_s.at[d], msem_r.at[d], dev))
        metas[-1].start()
    gt = jnp.where(slot_lane == group * trow + rank_g, 1.0, 0.0)
    gather = gt.T.astype(jnp.bfloat16)
    gt = gt.astype(jnp.bfloat16)

    for m in hop2:
        m.wait_recv()
    state = jnp.zeros((part, keys), jnp.float32)
    for g in range(groups - 1):
        step = factor_of(grecv[g, part : part + 16, :])
        state = jnp.where(me_g > g, step * state + grecv[g, 0:part, :].astype(jnp.float32), state)
    for j in range(quad):
        epack[j] = (before_decay[j] * state + before_state[j]).astype(jnp.bfloat16)
    hop3 = []
    mine_v = pl.ds(pl.multiple_of(me_q * part, part), part)
    for d in range(1, quad):
        j, dev = side(d)
        hop3.append(remote(epack.at[j], ent.at[mine_v], ms3.at[d], mr3.at[d], dev))
        hop3[-1].start()
    ent[mine_v, :] = epack[me_q]
    for m in hop3:
        m.wait_recv()
    scans = hop1 + hop2 + hop3
    entering = ent[...]

    def finish(which):
        at = pl.ds(pl.multiple_of(which * rows, rows), rows)
        for h in range(heads):
            pair = slice(h // 2 * 2 * KEY_DIM, (h // 2 + 1) * 2 * KEY_DIM)
            hv = slice(h * VALUE_DIM, (h + 1) * VALUE_DIM)
            attended = within[at, hv] + lax.dot_general(
                of_head(qlead[at, pair], h), entering[:, pair], nt,
                preferred_element_type=jnp.float32,
            )
            mean = jnp.mean(attended * attended, axis=1, keepdims=True)
            unit = attended * lax.rsqrt(mean + 1e-06) * hgain_ref[...]
            mix_ref[at, hv] = (unit * silu(og_ref[at, hv].astype(jnp.float32))).astype(
                jnp.bfloat16
            )

    other = 1 - me_tp
    finish(other)
    mixcopy = remote(
        mix_ref.at[pl.ds(pl.multiple_of(other * rows, rows), rows)], mixin,
        mixsem.at[0], mixsem.at[1], (me_sp, other),
    )
    mixcopy.start()

    finish(me_tp)

    weights[0].wait()
    own = mix_ref[pl.ds(pl.multiple_of(me_tp * rows, rows), rows), :]
    own_w = pl.multiple_of(me_tp * half, half)
    oth_w = pl.multiple_of(other * half, half)
    cols = [pl.ds(k * chunk, chunk) for k in range(CHUNKS)]
    part = [dot(own, wo[pl.ds(own_w, half), c]) for c in cols]
    mixcopy.wait_recv()
    peer = mixin[...]
    square = jnp.zeros((rows, 1), jnp.float32)
    for k, c in enumerate(cols):
        total = part[k] + dot(peer, wo[pl.ds(oth_w, half), c])
        summed = (res_ref[:, c].astype(jnp.float32) + total).astype(jnp.bfloat16)
        merged[:, c] = summed
        wide = summed.astype(jnp.float32)
        square = square + jnp.sum(wide * wide, axis=1, keepdims=True)
    inv = lax.rsqrt(square / width + 1e-06)
    for c in cols:
        normed[:, c] = (merged[:, c].astype(jnp.float32) * inv * gain_ref[:, c]).astype(
            jnp.bfloat16
        )

    if lanes > groups * trow:
        pad = lanes - groups * trow
        rbuf[pl.ds(groups * trow, pad), :] = jnp.zeros((pad, width), jnp.bfloat16)
        zrecv[pl.ds(groups * trow, pad), :] = jnp.zeros((pad, width), jnp.bfloat16)
    far_rows = lambda g: pl.ds(pl.multiple_of(g * trow, 16), trow)
    near_rows = lambda l: pl.ds(pl.multiple_of(l * erow, 16), erow)
    sends = [mixcopy] + metas + scans

    def spread_far(k, src, dst, ss, rr):
        out = []
        for d in range(1, groups):
            g, dev = far(d)
            out.append(
                remote(
                    src.at[far_rows(g), cols[k]], dst.at[far_rows(me_g), cols[k]],
                    ss.at[k, d], rr.at[k, d], dev,
                )
            )
            out[-1].start()
        dst[far_rows(me_g), cols[k]] = src[far_rows(me_g), cols[k]]
        return out

    def spread_near(k, src, dst, ss, rr):
        out = []
        for d in range(1, GROUP_SIZE):
            l, dev = near(d)
            out.append(
                remote(
                    src.at[near_rows(l), cols[k]], dst.at[near_rows(me_l), cols[k]],
                    ss.at[k, d], rr.at[k, d], dev,
                )
            )
            out[-1].start()
        dst[near_rows(me_l), cols[k]] = src[near_rows(me_l), cols[k]]
        return out

    first = []
    for k, c in enumerate(cols):
        sbuf[:, c] = dot(gather, normed[:, c]).astype(jnp.bfloat16)
        first.append(spread_far(k, sbuf, rbuf, s1, r1))

    for m in metas:
        m.wait_recv()
    table = mrecv[0]
    for g in range(1, groups):
        table = table + mrecv[g]
    key = lax.broadcasted_iota(jnp.int32, (GROUP_SIZE * erow, lanes), 0).astype(jnp.float32) + 1.0
    hit_a = key == table[0:1, :]
    hit_b = key == table[1:2, :]
    pick = (jnp.where(hit_a, 1.0, 0.0) + jnp.where(hit_b, 1.0, 0.0)).astype(jnp.bfloat16)

    second = []
    for k, c in enumerate(cols):
        for m in first[k]:
            m.wait_recv()
        xsend[:, c] = dot(pick, rbuf[:, c]).astype(jnp.bfloat16)
        second.append(spread_near(k, xsend, xin, s2, r2))

    blend = (jnp.where(hit_a, table[2:3, :], 0.0) + jnp.where(hit_b, table[3:4, :], 0.0)).T
    blend_hi = blend.astype(jnp.bfloat16)
    blend_lo = (blend - blend_hi.astype(jnp.float32)).astype(jnp.bfloat16)
    weights[1].wait()
    weights[2].wait()
    for k, c in enumerate(cols):
        for m in second[k]:
            m.wait_recv()
        block = xin[:, c]
        if k == 0:
            gacc[...] = dot(block, wg[c, :])
            uacc[...] = dot(block, wu[c, :])
        else:
            gacc[...] += dot(block, wg[c, :])
            uacc[...] += dot(block, wu[c, :])
    inner = (silu(gacc[...]) * uacc[...]).astype(jnp.bfloat16)
    weights[3].wait()
    third = []
    for k, c in enumerate(cols):
        ysend[:, c] = dot(inner, wd[:, c]).astype(jnp.bfloat16)
        third.append(spread_near(k, ysend, yrecv, s3, r3))
    fourth = []
    for k, c in enumerate(cols):
        for m in third[k]:
            m.wait_recv()
        block = yrecv[:, c]
        zsend[:, c] = (dot(blend_hi, block) + dot(blend_lo, block)).astype(jnp.bfloat16)
        fourth.append(spread_far(k, zsend, zrecv, s4, r4))
    for k, c in enumerate(cols):
        for m in fourth[k]:
            m.wait_recv()
        out_ref[:, c] = (merged[:, c].astype(jnp.float32) + dot(gt, zrecv[:, c])).astype(
            jnp.bfloat16
        )
    for batch in first + second + third + fourth:
        sends = sends + batch
    for m in sends:
        m.wait_send()


def rbuf_rows(rows, sp, tp):
    cap = 3 * rows // (sp * tp)
    most = min(GROUP_SIZE * cap // 2, rows)
    return -(-most // 16) * 16


def layer_call(
    q, k, v, og, gl, head_gain, residual, out_weight, norm_gain, routes, group_score, expert_score, wg, wu, wd
):
    sp, tp = lax.axis_size("sp"), lax.axis_size("tp")
    rows, width = residual.shape
    groups = sp * tp // GROUP_SIZE
    cap = 3 * rows // (sp * tp)
    lanes = -(-groups * rbuf_rows(rows, sp, tp) // 128) * 128
    erows = GROUP_SIZE * groups * cap
    hidden = wg.shape[1]
    quad = GROUP_SIZE // tp
    part = VALUE_DIM // quad
    keys = q.shape[1]
    vm = pl.BlockSpec(memory_space=pltpu.VMEM)
    hb = pl.BlockSpec(memory_space=pl.ANY)
    bf = jnp.bfloat16
    dma = pltpu.SemaphoreType.DMA
    fd, nd = (CHUNKS, groups), (CHUNKS, GROUP_SIZE)
    inputs = (
        gl, k, v, q, routes.T, group_score[None, :], expert_score.T,
        og, head_gain[None, :], residual, norm_gain[None, :],
    )
    return pl.pallas_call(
        functools.partial(layer_kernel, sp, tp),
        out_shape=pltpu.VMEM((rows, width), bf),
        in_specs=[hb] * 15,
        out_specs=vm,
        scratch_shapes=[
            *[pltpu.VMEM(x.shape, x.dtype) for x in inputs],
            pltpu.VMEM(out_weight.shape, bf),
            pltpu.VMEM(wg.shape, bf),
            pltpu.VMEM(wu.shape, bf),
            pltpu.VMEM(wd.shape, bf),
            pltpu.VMEM((rows, v.shape[1]), bf),
            pltpu.VMEM((rows, width), bf),
            pltpu.VMEM((rows, width), bf),
            pltpu.VMEM((lanes, width), bf),
            pltpu.VMEM((lanes, width), bf),
            pltpu.VMEM((erows, width), bf),
            pltpu.VMEM((erows, width), bf),
            pltpu.VMEM((erows, width), bf),
            pltpu.VMEM((erows, width), bf),
            pltpu.VMEM((lanes, width), bf),
            pltpu.VMEM((lanes, width), bf),
            pltpu.VMEM((groups, 8, lanes), jnp.float32),
            pltpu.VMEM((groups, 8, lanes), jnp.float32),
            pltpu.VMEM((erows, hidden), jnp.float32),
            pltpu.VMEM((erows, hidden), jnp.float32),
            pltpu.VMEM(v.shape, bf),
            pltpu.VMEM(q.shape, bf),
            pltpu.VMEM(v.shape, jnp.float32),
            pltpu.VMEM((quad, part + 16, keys), bf),
            pltpu.VMEM((quad, part + 16, keys), bf),
            pltpu.VMEM((part + 16, keys), bf),
            pltpu.VMEM((groups, part + 16, keys), bf),
            pltpu.VMEM((quad, part, keys), bf),
            pltpu.VMEM((VALUE_DIM, keys), bf),
            dma((quad,)), dma((quad,)), dma((groups,)), dma((groups,)), dma((quad,)), dma((quad,)),
            dma((15,)), dma((2,)), dma((groups,)), dma((groups,)),
            dma(fd), dma(fd), dma(nd), dma(nd), dma(nd), dma(nd), dma(fd), dma(fd),
        ],
        compiler_params=pltpu.CompilerParams(
            collective_id=0, has_side_effects=True, vmem_limit_bytes=60 * 1024 * 1024
        ),
    )(*inputs, out_weight, wg, wu, wd)


def local(
    residual,
    queries,
    key_rows,
    value_rows,
    out_gate,
    gate_logits,
    head_gain,
    out_weight,
    norm_gain,
    routes,
    group_score,
    expert_score,
    gate_weight,
    up_weight,
    down_weight,
):
    return layer_call(
        queries, key_rows, value_rows, out_gate, gate_logits, head_gain,
        residual, out_weight, norm_gain, routes, group_score, expert_score,
        gate_weight[0], up_weight[0], down_weight[0],
    )


def solution(mesh):
    placed = (
        P(("sp", "tp"), None),
        P("sp", "tp"),
        P("sp", "tp"),
        P("sp", "tp"),
        P("sp", "tp"),
        P("sp", "tp"),
        P(),
        P(),
        P(),
        P(("sp", "tp"), None),
        P(("sp", "tp")),
        P(("sp", "tp"), None),
        P(("sp", "tp"), None, None),
        P(("sp", "tp"), None, None),
        P(("sp", "tp"), None, None),
    )
    return jax.shard_map(
        local, mesh=mesh, in_specs=placed, out_specs=P(("sp", "tp"), None), check_vma=False
    )
```

```python
import functools

import jax
import jax.numpy as jnp
from jax import lax
from jax.experimental import pallas as pl
from jax.experimental.pallas import tpu as pltpu
from jax.sharding import PartitionSpec as P

KEY_DIM = 64
VALUE_DIM = 128
BLOCK = 64
GROUP_SIZE = 8
MESH = pl.DeviceIdType.MESH
CHUNKS = 4
UNITS = 4
TILE = 16


def dot(a, b):
    return jnp.dot(a, b, preferred_element_type=jnp.float32)


def silu(v):
    return v / (1.0 + jnp.exp(-v))


def layer_kernel(
    sp, tp, gl_hbm, k_hbm, v_hbm, q_hbm, routes_hbm, gscore_hbm, escore_hbm,
    og_hbm, hgain_hbm, res_hbm, gain_hbm, wo_hbm, wg_hbm, wu_hbm, wd_hbm, out_ref,
    gl_ref, k_ref, v_ref, q_ref, routes_ref, gscore_ref, escore_ref,
    og_ref, hgain_ref, res_ref, gain_ref, wo, wg, wu, wd, mixin, merged, normed, sbuf, rbuf, xsend, xin, ysend, yrecv, zsend, zrecv,
    msend, mrecv,
    mix_ref, qlead, within, spack, srecv, gpack, grecv, epack, ent,
    ms1, mr1, ms2, mr2, ms3, mr3, isem, mixsem, msem_s, msem_r, s1, r1, s2, r2, s3, r3, s4, r4,
):
    rows, width = res_ref.shape
    half = v_ref.shape[1]
    experts = sp * tp
    cap = 3 * rows // experts
    quad = GROUP_SIZE // tp
    groups = sp // quad
    trow = rbuf_rows(rows, sp, tp)
    per = groups // UNITS
    slots = per * cap
    bulk = width * slots // TILE
    narrow = width - bulk
    packs = bulk // narrow
    lanes = sbuf.shape[0]
    chunk = width // CHUNKS
    me_sp = lax.axis_index("sp")
    me_tp = lax.axis_index("tp")
    me_g = me_sp // quad
    me_q = me_sp % quad
    me_l = me_q * tp + me_tp

    pairs = (
        (gl_hbm, gl_ref), (k_hbm, k_ref), (v_hbm, v_ref), (q_hbm, q_ref),
        (routes_hbm, routes_ref), (gscore_hbm, gscore_ref), (escore_hbm, escore_ref),
        (og_hbm, og_ref), (hgain_hbm, hgain_ref), (res_hbm, res_ref), (gain_hbm, gain_ref),
        (wo_hbm, wo), (wg_hbm, wg), (wu_hbm, wu), (wd_hbm, wd),
    )
    loads = [pltpu.make_async_copy(h, v, isem.at[i]) for i, (h, v) in enumerate(pairs)]
    weights = loads[11:]

    def far(d):
        g = lax.rem(me_g + d, groups)
        return g, (g * quad + me_q, me_tp)

    def near(d):
        l = lax.rem(me_l + d, GROUP_SIZE)
        return l, (me_g * quad + l // tp, l % tp)

    barrier = pltpu.get_barrier_semaphore()
    for d in range(1, groups):
        pl.semaphore_signal(barrier, inc=1, device_id=far(d)[1], device_id_type=MESH)
    for d in range(1, GROUP_SIZE):
        pl.semaphore_signal(barrier, inc=1, device_id=near(d)[1], device_id_type=MESH)
    for w in loads:
        w.start()

    def remote(src, dst, ssem, rsem, dev):
        return pltpu.make_async_remote_copy(
            src_ref=src, dst_ref=dst, send_sem=ssem, recv_sem=rsem, device_id=dev,
            device_id_type=MESH,
        )

    length, keys = q_ref.shape
    heads = keys // KEY_DIM
    blocks = length // BLOCK
    part = VALUE_DIM // quad
    loads[0].wait()
    logits = gl_ref[...].astype(jnp.float32)
    logs = (jnp.minimum(logits, 0.0) - jnp.log1p(jnp.exp(-jnp.abs(logits)))) / 16.0
    pos_i = lax.broadcasted_iota(jnp.int32, (length, length), 0)
    pos_j = lax.broadcasted_iota(jnp.int32, (length, length), 1)
    causal = (pos_i // BLOCK == pos_j // BLOCK) & (pos_j <= pos_i)
    running = jnp.dot(
        jnp.where(causal, 1.0, 0.0), logs,
        preferred_element_type=jnp.float32, precision=lax.Precision.HIGHEST,
    )
    split = [slice(n * BLOCK, (n + 1) * BLOCK) for n in range(blocks)]
    closing = [running[(n + 1) * BLOCK - 1 : (n + 1) * BLOCK, :] for n in range(blocks)]
    loads[1].wait()
    key_float = k_ref[...].astype(jnp.float32)
    key_closing = [key_float[s] * jnp.exp(closing[n] - running[s]) for n, s in enumerate(split)]
    key_end = list(key_closing)
    tail = jnp.zeros_like(closing[0])
    for n in range(blocks - 1, -1, -1):
        if n < blocks - 1:
            key_end[n] = key_closing[n] * jnp.exp(tail)
        tail = tail + closing[n]
    key_end = jnp.concatenate(key_end, axis=0).astype(jnp.bfloat16)
    low = lax.broadcasted_iota(jnp.int32, (VALUE_DIM, 2 * KEY_DIM), 1) < KEY_DIM
    bf = jnp.bfloat16
    tile = lax.broadcasted_iota(jnp.int32, (16, keys), 0)

    def as_rows(factor):
        high = factor.astype(bf).astype(jnp.float32)
        return jnp.where(tile == 0, high, jnp.where(tile == 1, factor - high, 0.0)).astype(bf)

    def factor_of(rows16):
        wide = rows16.astype(jnp.float32)
        return wide[0:1] + wide[1:2]

    loads[2].wait()
    for p in range(heads // 2):
        pair = slice(p * 2 * KEY_DIM, (p + 1) * 2 * KEY_DIM)
        both = [
            lax.dot_general(
                v_ref[:, h * VALUE_DIM : (h + 1) * VALUE_DIM], key_end[:, pair],
                (((0,), (0,)), ((), ())), preferred_element_type=jnp.float32,
            )
            for h in (2 * p, 2 * p + 1)
        ]
        end = jnp.where(low, both[0], both[1])
        for j in range(quad):
            spack[j, 0:part, pair] = end[j * part : (j + 1) * part].astype(bf)
    decay_rows = as_rows(jnp.exp(tail))
    for j in range(quad):
        spack[j, part : part + 16, :] = decay_rows
    pl.semaphore_wait(barrier, groups - 1 + GROUP_SIZE - 1)

    def side(d):
        j = lax.rem(me_q + d, quad)
        return j, (me_g * quad + j, me_tp)

    hop1 = []
    for d in range(1, quad):
        j, dev = side(d)
        hop1.append(remote(spack.at[j], srecv.at[me_q], ms1.at[d], mr1.at[d], dev))
        hop1[-1].start()
    srecv[me_q] = spack[me_q]

    loads[3].wait()
    query = q_ref[...].astype(jnp.float32) * KEY_DIM ** (-0.5) * jnp.exp(running)
    key_inverse = (key_float * jnp.exp(-running)).astype(jnp.bfloat16)
    query_bf = query.astype(jnp.bfloat16)
    lead = jnp.zeros_like(closing[0])
    for n, s in enumerate(split):
        qlead[s, :] = (query[s] * jnp.exp(lead)).astype(jnp.bfloat16)
        lead = lead + closing[n]
    older = []
    for n in range(1, blocks):
        pieces = []
        gap = jnp.zeros_like(closing[0])
        for m in range(n - 1, -1, -1):
            pieces.insert(0, key_closing[m] if m == n - 1 else key_closing[m] * jnp.exp(gap))
            gap = gap + closing[m]
        pieces.append(jnp.zeros((length - n * BLOCK, keys), jnp.float32))
        older.append(jnp.concatenate(pieces, axis=0).astype(jnp.bfloat16))
    lane2 = lax.broadcasted_iota(jnp.int32, (length, 2 * KEY_DIM), 1)
    nt = (((1,), (1,)), ((), ()))

    def of_head(x, h):
        keep = lane2[: x.shape[0]] < KEY_DIM if h % 2 == 0 else lane2[: x.shape[0]] >= KEY_DIM
        return jnp.where(keep, x, jnp.zeros_like(x))

    for h in range(heads):
        pair = slice(h // 2 * 2 * KEY_DIM, (h // 2 + 1) * 2 * KEY_DIM)
        mine_q = of_head(query_bf[:, pair], h)
        score = lax.dot_general(
            mine_q, key_inverse[:, pair], nt, preferred_element_type=jnp.float32
        )
        past = [jnp.zeros((BLOCK, length), jnp.float32)]
        for n in range(1, blocks):
            past.append(
                lax.dot_general(
                    mine_q[split[n]], older[n - 1][:, pair], nt,
                    preferred_element_type=jnp.float32,
                )
            )
        score = jnp.where(causal, score, jnp.concatenate(past, axis=0)).astype(jnp.bfloat16)
        hv = slice(h * VALUE_DIM, (h + 1) * VALUE_DIM)
        within[:, hv] = dot(score, v_ref[:, hv])

    for m in hop1:
        m.wait_recv()
    total = jnp.zeros((part, keys), jnp.float32)
    total_decay = jnp.ones((1, keys), jnp.float32)
    before_state, before_decay = [], []
    for j in range(quad):
        before_state.append(total)
        before_decay.append(total_decay)
        step = factor_of(srecv[j, part : part + 16, :])
        total = step * total + srecv[j, 0:part, :].astype(jnp.float32)
        total_decay = total_decay * step
    gpack[0:part, :] = total.astype(bf)
    gpack[part : part + 16, :] = as_rows(total_decay)
    hop2 = []
    for d in range(1, groups):
        g, dev = far(d)
        hop2.append(remote(gpack, grecv.at[me_g], ms2.at[d], mr2.at[d], dev))
        hop2[-1].start()
    grecv[me_g] = gpack[...]

    for w in loads[4:11]:
        w.wait()
    sub = lax.broadcasted_iota(jnp.int32, (rows, rows), 0)
    route_t = routes_ref[...].astype(jnp.float32)
    score_t = escore_ref[...]
    scale_t = gscore_ref[...] * score_t / jnp.sum(score_t, axis=0, keepdims=True)
    columns = jnp.where(sub == 0, route_t[0:1, :], 0.0) + jnp.where(sub == 1, route_t[1:2, :], 0.0)
    columns = columns.T
    ra = columns[:, 0:1].astype(jnp.int32)
    rb = columns[:, 1:2].astype(jnp.int32)
    elane = lax.broadcasted_iota(jnp.int32, (rows, 128), 1)
    row_i = lax.broadcasted_iota(jnp.int32, (rows, rows), 0)
    col_i = lax.broadcasted_iota(jnp.int32, (rows, rows), 1)
    strict = jnp.where(col_i < row_i, 1.0, 0.0).astype(jnp.bfloat16)
    is_a = elane == ra
    is_b = elane == rb
    either = (jnp.where(is_a, 1.0, 0.0) + jnp.where(is_b, 1.0, 0.0)).astype(jnp.bfloat16)
    before = dot(strict, either)
    rank_a = jnp.sum(jnp.where(is_a, before, 0.0), axis=1, keepdims=True)
    rank_b = jnp.sum(jnp.where(is_b, before, 0.0), axis=1, keepdims=True)
    group = ra // GROUP_SIZE
    is_g = elane == group
    before_g = dot(strict, jnp.where(is_g, 1.0, 0.0).astype(jnp.bfloat16))
    rank_g = jnp.sum(jnp.where(is_g, before_g, 0.0), axis=1, keepdims=True).astype(jnp.int32)
    code_a = ((ra % GROUP_SIZE) * cap + 1).astype(jnp.float32) + rank_a
    code_b = ((rb % GROUP_SIZE) * cap + 1).astype(jnp.float32) + rank_b
    values = jnp.where(elane == 0, code_a, 0.0) + jnp.where(elane == 1, code_b, 0.0)
    values_t = values.T[0:8, :]
    sub8 = lax.broadcasted_iota(jnp.int32, (8, rows), 0)
    values_t = values_t + jnp.where(sub8 == 2, scale_t[0:1, :], 0.0)
    values_t = values_t + jnp.where(sub8 == 3, scale_t[1:2, :], 0.0)
    slot_lane = lax.broadcasted_iota(jnp.int32, (rows, lanes), 1)
    mine = jnp.where(elane == rank_g, 1.0, 0.0)
    for g in range(groups):
        msend[g] = jnp.dot(
            values_t, jnp.where(group == g, mine, 0.0),
            preferred_element_type=jnp.float32, precision=lax.Precision.HIGHEST,
        )
    mrecv[me_g] = msend[me_g]
    metas = []
    for d in range(1, groups):
        g, dev = far(d)
        metas.append(remote(msend.at[g], mrecv.at[me_g], msem_s.at[d], msem_r.at[d], dev))
        metas[-1].start()
    gt = jnp.where(slot_lane == group * trow + rank_g, 1.0, 0.0)
    gather = gt.T.astype(jnp.bfloat16)
    gt = gt.astype(jnp.bfloat16)

    for m in hop2:
        m.wait_recv()
    state = jnp.zeros((part, keys), jnp.float32)
    for g in range(groups - 1):
        step = factor_of(grecv[g, part : part + 16, :])
        state = jnp.where(me_g > g, step * state + grecv[g, 0:part, :].astype(jnp.float32), state)
    for j in range(quad):
        epack[j] = (before_decay[j] * state + before_state[j]).astype(jnp.bfloat16)
    hop3 = []
    mine_v = pl.ds(pl.multiple_of(me_q * part, part), part)
    for d in range(1, quad):
        j, dev = side(d)
        hop3.append(remote(epack.at[j], ent.at[mine_v], ms3.at[d], mr3.at[d], dev))
        hop3[-1].start()
    ent[mine_v, :] = epack[me_q]
    for m in hop3:
        m.wait_recv()
    scans = hop1 + hop2 + hop3
    entering = ent[...]

    def finish(which):
        at = pl.ds(pl.multiple_of(which * rows, rows), rows)
        for h in range(heads):
            pair = slice(h // 2 * 2 * KEY_DIM, (h // 2 + 1) * 2 * KEY_DIM)
            hv = slice(h * VALUE_DIM, (h + 1) * VALUE_DIM)
            attended = within[at, hv] + lax.dot_general(
                of_head(qlead[at, pair], h), entering[:, pair], nt,
                preferred_element_type=jnp.float32,
            )
            mean = jnp.mean(attended * attended, axis=1, keepdims=True)
            unit = attended * lax.rsqrt(mean + 1e-06) * hgain_ref[...]
            mix_ref[at, hv] = (unit * silu(og_ref[at, hv].astype(jnp.float32))).astype(
                jnp.bfloat16
            )

    other = 1 - me_tp
    finish(other)
    mixcopy = remote(
        mix_ref.at[pl.ds(pl.multiple_of(other * rows, rows), rows)], mixin,
        mixsem.at[0], mixsem.at[1], (me_sp, other),
    )
    mixcopy.start()

    finish(me_tp)

    weights[0].wait()
    own = mix_ref[pl.ds(pl.multiple_of(me_tp * rows, rows), rows), :]
    own_w = pl.multiple_of(me_tp * half, half)
    oth_w = pl.multiple_of(other * half, half)
    cols = [pl.ds(k * chunk, chunk) for k in range(CHUNKS)]
    part = [dot(own, wo[pl.ds(own_w, half), c]) for c in cols]
    mixcopy.wait_recv()
    peer = mixin[...]
    square = jnp.zeros((rows, 1), jnp.float32)
    for k, c in enumerate(cols):
        total = part[k] + dot(peer, wo[pl.ds(oth_w, half), c])
        summed = (res_ref[:, c].astype(jnp.float32) + total).astype(jnp.bfloat16)
        merged[:, c] = summed
        wide = summed.astype(jnp.float32)
        square = square + jnp.sum(wide * wide, axis=1, keepdims=True)
    inv = lax.rsqrt(square / width + 1e-06)
    for c in cols:
        normed[:, c] = (merged[:, c].astype(jnp.float32) * inv * gain_ref[:, c]).astype(
            jnp.bfloat16
        )

    if lanes > groups * trow:
        pad = lanes - groups * trow
        zrecv[pl.ds(groups * trow, pad), :] = jnp.zeros((pad, width), bf)
    far_rows = lambda g: pl.ds(pl.multiple_of(g * trow, 16), trow)
    near_rows = lambda l: pl.ds(pl.multiple_of(l * TILE, TILE), TILE)
    sends = [mixcopy] + metas + scans
    order = arrival_order(me_g, groups)

    def home(g):
        return (g * quad + me_q, me_tp)

    def from_far(i):
        return remote(
            sbuf.at[far_rows(order[i])], rbuf.at[far_rows(order[i])],
            s1.at[i], r1.at[order[i]], home(order[i]),
        )

    sbuf[...] = dot(gather, normed[...]).astype(bf)
    for i, g in enumerate(send_order(me_g, groups)):
        sends.append(
            remote(
                sbuf.at[far_rows(g)], rbuf.at[far_rows(me_g)], s1.at[i], r1.at[me_g], home(g)
            )
        )
        sends[-1].start()
    rbuf[far_rows(me_g), :] = sbuf[far_rows(me_g), :]
    for m in metas:
        m.wait_recv()

    slab = GROUP_SIZE * TILE
    parts = [pl.ds(t * narrow, narrow) for t in range(packs)]
    last = pl.ds(bulk, narrow)

    def keys_of(row, t, p):
        at = row % TILE
        slot = at if t is None else packs * (at - slots) + t
        valid = at < slots if t is None else at >= slots
        if per > 1:
            valid = valid & (slot // cap == p)
        return jnp.where(valid, (row // TILE) * cap + slot - p * cap + 1, -1).astype(jnp.float32)

    down_row = lax.broadcasted_iota(jnp.int32, (slab, trow), 0)
    across_row = lax.broadcasted_iota(jnp.int32, (trow, slab), 1)
    sq_i = lax.broadcasted_iota(jnp.int32, (slab, slab), 0)
    sq_j = lax.broadcasted_iota(jnp.int32, (slab, slab), 1)

    def pairs_of(packed, plain, t):
        same = packed // TILE == plain // TILE
        at = packed % TILE
        hit = same & (at >= slots) & (plain % TILE == packs * (at - slots) + t)
        return jnp.where(hit & (plain % TILE < slots), 1.0, 0.0).astype(bf)

    unpack = [pairs_of(sq_j, sq_i, t) for t in range(packs)]
    repack = [pairs_of(sq_i, sq_j, t) for t in range(packs)]
    plain_row = lax.broadcasted_iota(jnp.int32, (slab, narrow), 0) % TILE < slots

    def spread(u, src, dst, ss, rr):
        out = []
        for d in range(1, GROUP_SIZE):
            l, dev = near(d)
            out.append(
                remote(
                    src.at[u, near_rows(l)], dst.at[u, near_rows(me_l)],
                    ss.at[u, d], rr.at[u, d], dev,
                )
            )
            out[-1].start()
        dst[u, near_rows(me_l), :] = src[u, near_rows(me_l), :]
        sends.extend(out)
        return out

    def dispatch(u):
        acc = [jnp.zeros((slab, narrow), jnp.float32) for _ in range(packs)]
        for p in range(per):
            i = u * per + p
            if i > 0:
                from_far(i).wait_recv()
            table = mrecv[order[i]][:, 0:trow]

            def pick(t):
                key = keys_of(down_row, t, p)
                hit = (key == table[0:1, :]) | (key == table[1:2, :])
                return jnp.where(hit, 1.0, 0.0).astype(bf)

            plain = pick(None)
            tail_cols = rbuf[far_rows(order[i]), last]
            for t in range(packs):
                acc[t] = acc[t] + dot(plain, rbuf[far_rows(order[i]), parts[t]])
                acc[t] = acc[t] + dot(pick(t), tail_cols)
        for t in range(packs):
            xsend[u, :, parts[t]] = acc[t].astype(bf)
        return spread(u, xsend, xin, s2, r2)

    def experts(u, arriving):
        for m in arriving:
            m.wait_recv()
        block = xin[u]
        rest = jnp.zeros((slab, narrow), jnp.float32)
        for t in range(packs):
            rest = rest + dot(unpack[t], xin[u, :, parts[t]])
        rest = rest.astype(bf)
        gated = dot(block, wg[0:bulk, :]) + dot(rest, wg[bulk:width, :])
        lifted = dot(block, wu[0:bulk, :]) + dot(rest, wu[bulk:width, :])
        inner = (silu(gated) * lifted).astype(bf)
        ends = dot(inner, wd[:, last]).astype(bf)
        for t in range(packs):
            main = dot(inner, wd[:, parts[t]])
            ysend[u, :, parts[t]] = jnp.where(plain_row, main, dot(repack[t], ends)).astype(bf)

    def give_back(u):
        return spread(u, ysend, yrecv, s3, r3)

    def combine(u, arriving):
        for m in arriving:
            m.wait_recv()
        for p in range(per):
            i = u * per + p
            table = mrecv[order[i]].T[0:trow, :]

            def blend(t):
                key = keys_of(across_row, t, p)
                both = jnp.where(key == table[:, 0:1], table[:, 2:3], 0.0)
                both = both + jnp.where(key == table[:, 1:2], table[:, 3:4], 0.0)
                high = both.astype(bf)
                return [high, (both - high.astype(jnp.float32)).astype(bf)]

            plain = blend(None)
            ends = jnp.zeros((trow, narrow), jnp.float32)
            to = zrecv if i == 0 else zsend
            for t in range(packs):
                four = dot(jnp.concatenate(plain + blend(t), axis=0), yrecv[u, :, parts[t]])
                to[far_rows(order[i]), parts[t]] = (four[0:trow] + four[trow : 2 * trow]).astype(bf)
                ends = ends + four[2 * trow : 3 * trow] + four[3 * trow : 4 * trow]
            to[far_rows(order[i]), last] = ends.astype(bf)
            if i > 0:
                sends.append(
                    remote(
                        zsend.at[far_rows(order[i])], zrecv.at[far_rows(me_g)],
                        s4.at[i], r4.at[me_g], home(order[i]),
                    )
                )
                sends[-1].start()

    out0 = dispatch(0)
    weights[1].wait()
    weights[2].wait()
    weights[3].wait()
    experts(0, out0)
    out1 = dispatch(1)
    out2 = dispatch(2)
    experts(1, out1)
    out3 = dispatch(3)
    back1 = give_back(1)
    experts(2, out2)
    back2 = give_back(2)
    experts(3, out3)
    back3 = give_back(3)
    back0 = give_back(0)
    combine(1, back1)
    combine(2, back2)
    combine(3, back3)
    combine(0, back0)
    for i in range(1, groups):
        g = order[i]
        remote(
            zsend.at[far_rows(g)], zrecv.at[far_rows(g)], s4.at[i], r4.at[g], home(g)
        ).wait_recv()
    for c in cols:
        out_ref[:, c] = (merged[:, c].astype(jnp.float32) + dot(gt, zrecv[:, c])).astype(bf)
    for m in sends:
        m.wait_send()


def by_place(me, rows):
    odd, high = me % 2, me // 2
    ones = [(1 - odd) * (1 - high), odd * (1 - high), (1 - odd) * high, odd * high]
    return [sum(one * row[i] for one, row in zip(ones, rows)) for i in range(len(rows[0]))]


def send_order(me, count):
    if count != 4:
        return [lax.rem(me + d, count) for d in range(1, count)]
    return by_place(me, ((3, 1, 2), (3, 2, 0), (0, 1, 3), (0, 2, 1)))


def arrival_order(me, count):
    if count != 4:
        return [me] + [lax.rem(me + count - d, count) for d in range(1, count)]
    return [me] + by_place(me, ((3, 2, 1), (0, 3, 2), (3, 0, 1), (0, 1, 2)))


def rbuf_rows(rows, sp, tp):
    cap = 3 * rows // (sp * tp)
    most = min(GROUP_SIZE * cap // 2, rows)
    return -(-most // 16) * 16


def layer_call(
    q, k, v, og, gl, head_gain, residual, out_weight, norm_gain, routes, group_score, expert_score, wg, wu, wd
):
    sp, tp = lax.axis_size("sp"), lax.axis_size("tp")
    rows, width = residual.shape
    groups = sp * tp // GROUP_SIZE
    cap = 3 * rows // (sp * tp)
    lanes = -(-groups * rbuf_rows(rows, sp, tp) // 128) * 128
    slab = (UNITS, GROUP_SIZE * TILE, width * (groups // UNITS) * cap // TILE)
    quad = GROUP_SIZE // tp
    part = VALUE_DIM // quad
    keys = q.shape[1]
    vm = pl.BlockSpec(memory_space=pltpu.VMEM)
    hb = pl.BlockSpec(memory_space=pl.ANY)
    bf = jnp.bfloat16
    dma = pltpu.SemaphoreType.DMA
    fd, nd = (groups,), (UNITS, GROUP_SIZE)
    inputs = (
        gl, k, v, q, routes.T, group_score[None, :], expert_score.T,
        og, head_gain[None, :], residual, norm_gain[None, :],
    )
    return pl.pallas_call(
        functools.partial(layer_kernel, sp, tp),
        out_shape=pltpu.VMEM((rows, width), bf),
        in_specs=[hb] * 15,
        out_specs=vm,
        scratch_shapes=[
            *[pltpu.VMEM(x.shape, x.dtype) for x in inputs],
            pltpu.VMEM(out_weight.shape, bf),
            pltpu.VMEM(wg.shape, bf),
            pltpu.VMEM(wu.shape, bf),
            pltpu.VMEM(wd.shape, bf),
            pltpu.VMEM((rows, v.shape[1]), bf),
            pltpu.VMEM((rows, width), bf),
            pltpu.VMEM((rows, width), bf),
            pltpu.VMEM((lanes, width), bf),
            pltpu.VMEM((lanes, width), bf),
            pltpu.VMEM(slab, bf),
            pltpu.VMEM(slab, bf),
            pltpu.VMEM(slab, bf),
            pltpu.VMEM(slab, bf),
            pltpu.VMEM((lanes, width), bf),
            pltpu.VMEM((lanes, width), bf),
            pltpu.VMEM((groups, 8, 128), jnp.float32),
            pltpu.VMEM((groups, 8, 128), jnp.float32),
            pltpu.VMEM(v.shape, bf),
            pltpu.VMEM(q.shape, bf),
            pltpu.VMEM(v.shape, jnp.float32),
            pltpu.VMEM((quad, part + 16, keys), bf),
            pltpu.VMEM((quad, part + 16, keys), bf),
            pltpu.VMEM((part + 16, keys), bf),
            pltpu.VMEM((groups, part + 16, keys), bf),
            pltpu.VMEM((quad, part, keys), bf),
            pltpu.VMEM((VALUE_DIM, keys), bf),
            dma((quad,)), dma((quad,)), dma((groups,)), dma((groups,)), dma((quad,)), dma((quad,)),
            dma((15,)), dma((2,)), dma((groups,)), dma((groups,)),
            dma(fd), dma(fd), dma(nd), dma(nd), dma(nd), dma(nd), dma(fd), dma(fd),
        ],
        compiler_params=pltpu.CompilerParams(
            collective_id=0, has_side_effects=True, vmem_limit_bytes=60 * 1024 * 1024
        ),
    )(*inputs, out_weight, wg, wu, wd)


def local(
    residual,
    queries,
    key_rows,
    value_rows,
    out_gate,
    gate_logits,
    head_gain,
    out_weight,
    norm_gain,
    routes,
    group_score,
    expert_score,
    gate_weight,
    up_weight,
    down_weight,
):
    return layer_call(
        queries, key_rows, value_rows, out_gate, gate_logits, head_gain,
        residual, out_weight, norm_gain, routes, group_score, expert_score,
        gate_weight[0], up_weight[0], down_weight[0],
    )


def solution(mesh):
    placed = (
        P(("sp", "tp"), None),
        P("sp", "tp"),
        P("sp", "tp"),
        P("sp", "tp"),
        P("sp", "tp"),
        P("sp", "tp"),
        P(),
        P(),
        P(),
        P(("sp", "tp"), None),
        P(("sp", "tp")),
        P(("sp", "tp"), None),
        P(("sp", "tp"), None, None),
        P(("sp", "tp"), None, None),
        P(("sp", "tp"), None, None),
    )
    return jax.shard_map(
        local, mesh=mesh, in_specs=placed, out_specs=P(("sp", "tp"), None), check_vma=False
    )
```

```python
import functools

import jax
import jax.numpy as jnp
from jax import lax
from jax.experimental import pallas as pl
from jax.experimental.pallas import tpu as pltpu
from jax.sharding import PartitionSpec as P

KEY_DIM = 64
VALUE_DIM = 128
BLOCK = 64
GROUP_SIZE = 8
MESH = pl.DeviceIdType.MESH
CHUNKS = 4
UNITS = 4
TILE = 16


def dot(a, b):
    return jnp.dot(a, b, preferred_element_type=jnp.float32)


def silu(v):
    return v / (1.0 + jnp.exp(-v))


def layer_kernel(
    sp, tp, gl_hbm, k_hbm, v_hbm, q_hbm, routes_hbm, gscore_hbm, escore_hbm,
    og_hbm, hgain_hbm, res_hbm, gain_hbm, wo_hbm, wg_hbm, wu_hbm, wd_hbm, out_ref,
    gl_ref, k_ref, v_ref, q_ref, routes_ref, gscore_ref, escore_ref,
    og_ref, hgain_ref, res_ref, gain_ref, wo, wg, wu, wd, mixin, merged, normed, sbuf, rbuf, xsend, xin, ysend, yrecv, zsend, zrecv,
    msend, mrecv,
    mix_ref, qlead, within, spack, srecv, gpack, grecv, epack, ent,
    ms1, mr1, ms2, mr2, ms3, mr3, isem, mixsem, msem_s, msem_r, s1, r1, s2, r2, s3, r3, s4, r4,
):
    rows, width = res_ref.shape
    half = v_ref.shape[1]
    experts = sp * tp
    cap = 3 * rows // experts
    quad = GROUP_SIZE // tp
    groups = sp // quad
    trow = rbuf_rows(rows, sp, tp)
    per = groups // UNITS
    slots = per * cap
    bulk = width * slots // TILE
    narrow = width - bulk
    packs = bulk // narrow
    lanes = sbuf.shape[0]
    chunk = width // CHUNKS
    me_sp = lax.axis_index("sp")
    me_tp = lax.axis_index("tp")
    me_g = me_sp // quad
    me_q = me_sp % quad
    me_l = me_q * tp + me_tp

    pairs = (
        (gl_hbm, gl_ref), (k_hbm, k_ref), (v_hbm, v_ref), (q_hbm, q_ref),
        (routes_hbm, routes_ref), (gscore_hbm, gscore_ref), (escore_hbm, escore_ref),
        (og_hbm, og_ref), (hgain_hbm, hgain_ref), (res_hbm, res_ref), (gain_hbm, gain_ref),
        (wo_hbm, wo), (wg_hbm, wg), (wu_hbm, wu), (wd_hbm, wd),
    )
    loads = [pltpu.make_async_copy(h, v, isem.at[i]) for i, (h, v) in enumerate(pairs)]
    weights = loads[11:]

    def far(d):
        g = lax.rem(me_g + d, groups)
        return g, (g * quad + me_q, me_tp)

    def near(d):
        l = lax.rem(me_l + d, GROUP_SIZE)
        return l, (me_g * quad + l // tp, l % tp)

    barrier = pltpu.get_barrier_semaphore()
    for d in range(1, groups):
        pl.semaphore_signal(barrier, inc=1, device_id=far(d)[1], device_id_type=MESH)
    for d in range(1, GROUP_SIZE):
        pl.semaphore_signal(barrier, inc=1, device_id=near(d)[1], device_id_type=MESH)
    for w in loads:
        w.start()

    def remote(src, dst, ssem, rsem, dev):
        return pltpu.make_async_remote_copy(
            src_ref=src, dst_ref=dst, send_sem=ssem, recv_sem=rsem, device_id=dev,
            device_id_type=MESH,
        )

    length, keys = q_ref.shape
    heads = keys // KEY_DIM
    blocks = length // BLOCK
    part = VALUE_DIM // quad
    loads[0].wait()
    logits = gl_ref[...].astype(jnp.float32)
    logs = (jnp.minimum(logits, 0.0) - jnp.log1p(jnp.exp(-jnp.abs(logits)))) / 16.0
    pos_i = lax.broadcasted_iota(jnp.int32, (length, length), 0)
    pos_j = lax.broadcasted_iota(jnp.int32, (length, length), 1)
    causal = (pos_i // BLOCK == pos_j // BLOCK) & (pos_j <= pos_i)
    running = jnp.dot(
        jnp.where(causal, 1.0, 0.0), logs,
        preferred_element_type=jnp.float32, precision=lax.Precision.HIGHEST,
    )
    split = [slice(n * BLOCK, (n + 1) * BLOCK) for n in range(blocks)]
    closing = [running[(n + 1) * BLOCK - 1 : (n + 1) * BLOCK, :] for n in range(blocks)]
    loads[1].wait()
    key_float = k_ref[...].astype(jnp.float32)
    key_closing = [key_float[s] * jnp.exp(closing[n] - running[s]) for n, s in enumerate(split)]
    key_end = list(key_closing)
    tail = jnp.zeros_like(closing[0])
    for n in range(blocks - 1, -1, -1):
        if n < blocks - 1:
            key_end[n] = key_closing[n] * jnp.exp(tail)
        tail = tail + closing[n]
    key_end = jnp.concatenate(key_end, axis=0).astype(jnp.bfloat16)
    low = lax.broadcasted_iota(jnp.int32, (VALUE_DIM, 2 * KEY_DIM), 1) < KEY_DIM
    bf = jnp.bfloat16
    tile = lax.broadcasted_iota(jnp.int32, (16, keys), 0)

    def as_rows(factor):
        high = factor.astype(bf).astype(jnp.float32)
        return jnp.where(tile == 0, high, jnp.where(tile == 1, factor - high, 0.0)).astype(bf)

    def factor_of(rows16):
        wide = rows16.astype(jnp.float32)
        return wide[0:1] + wide[1:2]

    loads[2].wait()
    for p in range(heads // 2):
        pair = slice(p * 2 * KEY_DIM, (p + 1) * 2 * KEY_DIM)
        both = [
            lax.dot_general(
                v_ref[:, h * VALUE_DIM : (h + 1) * VALUE_DIM], key_end[:, pair],
                (((0,), (0,)), ((), ())), preferred_element_type=jnp.float32,
            )
            for h in (2 * p, 2 * p + 1)
        ]
        end = jnp.where(low, both[0], both[1])
        for j in range(quad):
            spack[j, 0:part, pair] = end[j * part : (j + 1) * part].astype(bf)
    decay_rows = as_rows(jnp.exp(tail))
    for j in range(quad):
        spack[j, part : part + 16, :] = decay_rows
    pl.semaphore_wait(barrier, groups - 1 + GROUP_SIZE - 1)

    def side(d):
        j = lax.rem(me_q + d, quad)
        return j, (me_g * quad + j, me_tp)

    beside = side(1)[1]

    def batch(src, dst, ss, rr):
        return remote(src, dst, ss, rr, beside)

    for d in range(1, quad):
        j, dev = side(d)
        remote(spack.at[j], srecv.at[me_q], ms1.at[0], mr1.at[0], dev).start()
    others = pl.ds(0, quad - 1)
    hop1 = batch(spack.at[others], srecv.at[others], ms1.at[0], mr1.at[0])
    srecv[me_q] = spack[me_q]

    loads[3].wait()
    query = q_ref[...].astype(jnp.float32) * KEY_DIM ** (-0.5) * jnp.exp(running)
    key_inverse = (key_float * jnp.exp(-running)).astype(jnp.bfloat16)
    query_bf = query.astype(jnp.bfloat16)
    lead = jnp.zeros_like(closing[0])
    for n, s in enumerate(split):
        qlead[s, :] = (query[s] * jnp.exp(lead)).astype(jnp.bfloat16)
        lead = lead + closing[n]
    older = []
    for n in range(1, blocks):
        pieces = []
        gap = jnp.zeros_like(closing[0])
        for m in range(n - 1, -1, -1):
            pieces.insert(0, key_closing[m] if m == n - 1 else key_closing[m] * jnp.exp(gap))
            gap = gap + closing[m]
        pieces.append(jnp.zeros((length - n * BLOCK, keys), jnp.float32))
        older.append(jnp.concatenate(pieces, axis=0).astype(jnp.bfloat16))
    lane2 = lax.broadcasted_iota(jnp.int32, (length, 2 * KEY_DIM), 1)
    nt = (((1,), (1,)), ((), ()))

    def of_head(x, h):
        keep = lane2[: x.shape[0]] < KEY_DIM if h % 2 == 0 else lane2[: x.shape[0]] >= KEY_DIM
        return jnp.where(keep, x, jnp.zeros_like(x))

    for h in range(heads):
        pair = slice(h // 2 * 2 * KEY_DIM, (h // 2 + 1) * 2 * KEY_DIM)
        mine_q = of_head(query_bf[:, pair], h)
        score = lax.dot_general(
            mine_q, key_inverse[:, pair], nt, preferred_element_type=jnp.float32
        )
        past = [jnp.zeros((BLOCK, length), jnp.float32)]
        for n in range(1, blocks):
            past.append(
                lax.dot_general(
                    mine_q[split[n]], older[n - 1][:, pair], nt,
                    preferred_element_type=jnp.float32,
                )
            )
        score = jnp.where(causal, score, jnp.concatenate(past, axis=0)).astype(jnp.bfloat16)
        hv = slice(h * VALUE_DIM, (h + 1) * VALUE_DIM)
        within[:, hv] = dot(score, v_ref[:, hv])

    hop1.wait_recv()
    total = jnp.zeros((part, keys), jnp.float32)
    total_decay = jnp.ones((1, keys), jnp.float32)
    before_state, before_decay = [], []
    for j in range(quad):
        before_state.append(total)
        before_decay.append(total_decay)
        step = factor_of(srecv[j, part : part + 16, :])
        total = step * total + srecv[j, 0:part, :].astype(jnp.float32)
        total_decay = total_decay * step
    gpack[0:part, :] = total.astype(bf)
    gpack[part : part + 16, :] = as_rows(total_decay)
    for d in range(1, groups):
        g, dev = far(d)
        remote(gpack, grecv.at[me_g], ms2.at[0], mr2.at[0], dev).start()
    apart = pl.ds(0, groups - 1)
    hop2 = batch(grecv.at[apart], grecv.at[apart], ms2.at[0], mr2.at[0])
    grecv[me_g] = gpack[...]

    for w in loads[4:11]:
        w.wait()
    sub = lax.broadcasted_iota(jnp.int32, (rows, rows), 0)
    route_t = routes_ref[...].astype(jnp.float32)
    score_t = escore_ref[...]
    scale_t = gscore_ref[...] * score_t / jnp.sum(score_t, axis=0, keepdims=True)
    columns = jnp.where(sub == 0, route_t[0:1, :], 0.0) + jnp.where(sub == 1, route_t[1:2, :], 0.0)
    columns = columns.T
    ra = columns[:, 0:1].astype(jnp.int32)
    rb = columns[:, 1:2].astype(jnp.int32)
    elane = lax.broadcasted_iota(jnp.int32, (rows, 128), 1)
    row_i = lax.broadcasted_iota(jnp.int32, (rows, rows), 0)
    col_i = lax.broadcasted_iota(jnp.int32, (rows, rows), 1)
    strict = jnp.where(col_i < row_i, 1.0, 0.0).astype(jnp.bfloat16)
    is_a = elane == ra
    is_b = elane == rb
    either = (jnp.where(is_a, 1.0, 0.0) + jnp.where(is_b, 1.0, 0.0)).astype(jnp.bfloat16)
    before = dot(strict, either)
    rank_a = jnp.sum(jnp.where(is_a, before, 0.0), axis=1, keepdims=True)
    rank_b = jnp.sum(jnp.where(is_b, before, 0.0), axis=1, keepdims=True)
    group = ra // GROUP_SIZE
    is_g = elane == group
    before_g = dot(strict, jnp.where(is_g, 1.0, 0.0).astype(jnp.bfloat16))
    rank_g = jnp.sum(jnp.where(is_g, before_g, 0.0), axis=1, keepdims=True).astype(jnp.int32)
    code_a = ((ra % GROUP_SIZE) * cap + 1).astype(jnp.float32) + rank_a
    code_b = ((rb % GROUP_SIZE) * cap + 1).astype(jnp.float32) + rank_b
    values = jnp.where(elane == 0, code_a, 0.0) + jnp.where(elane == 1, code_b, 0.0)
    values_t = values.T[0:8, :]
    sub8 = lax.broadcasted_iota(jnp.int32, (8, rows), 0)
    values_t = values_t + jnp.where(sub8 == 2, scale_t[0:1, :], 0.0)
    values_t = values_t + jnp.where(sub8 == 3, scale_t[1:2, :], 0.0)
    slot_lane = lax.broadcasted_iota(jnp.int32, (rows, lanes), 1)
    mine = jnp.where(elane == rank_g, 1.0, 0.0)
    for g in range(groups):
        msend[g] = jnp.dot(
            values_t, jnp.where(group == g, mine, 0.0),
            preferred_element_type=jnp.float32, precision=lax.Precision.HIGHEST,
        )
    mrecv[me_g] = msend[me_g]
    for d in range(1, groups):
        g, dev = far(d)
        remote(msend.at[g], mrecv.at[me_g], msem_s.at[0], msem_r.at[0], dev).start()
    metas = batch(msend.at[apart], mrecv.at[apart], msem_s.at[0], msem_r.at[0])
    gt = jnp.where(slot_lane == group * trow + rank_g, 1.0, 0.0)
    gather = gt.T.astype(jnp.bfloat16)
    gt = gt.astype(jnp.bfloat16)

    hop2.wait_recv()
    state = jnp.zeros((part, keys), jnp.float32)
    for g in range(groups - 1):
        step = factor_of(grecv[g, part : part + 16, :])
        state = jnp.where(me_g > g, step * state + grecv[g, 0:part, :].astype(jnp.float32), state)
    for j in range(quad):
        epack[j] = (before_decay[j] * state + before_state[j]).astype(jnp.bfloat16)
    mine_v = pl.ds(pl.multiple_of(me_q * part, part), part)
    for d in range(1, quad):
        j, dev = side(d)
        remote(epack.at[j], ent.at[mine_v], ms3.at[0], mr3.at[0], dev).start()
    ent[mine_v, :] = epack[me_q]
    slices = pl.ds(0, (quad - 1) * part)
    hop3 = batch(ent.at[slices], ent.at[slices], ms3.at[0], mr3.at[0])
    hop3.wait_recv()
    sends = [hop1, hop2, hop3, metas]
    entering = ent[...]

    def finish(which):
        at = pl.ds(pl.multiple_of(which * rows, rows), rows)
        for h in range(heads):
            pair = slice(h // 2 * 2 * KEY_DIM, (h // 2 + 1) * 2 * KEY_DIM)
            hv = slice(h * VALUE_DIM, (h + 1) * VALUE_DIM)
            attended = within[at, hv] + lax.dot_general(
                of_head(qlead[at, pair], h), entering[:, pair], nt,
                preferred_element_type=jnp.float32,
            )
            mean = jnp.mean(attended * attended, axis=1, keepdims=True)
            unit = attended * lax.rsqrt(mean + 1e-06) * hgain_ref[...]
            mix_ref[at, hv] = (unit * silu(og_ref[at, hv].astype(jnp.float32))).astype(
                jnp.bfloat16
            )

    other = 1 - me_tp
    finish(other)
    mixcopy = remote(
        mix_ref.at[pl.ds(pl.multiple_of(other * rows, rows), rows)], mixin,
        mixsem.at[0], mixsem.at[1], (me_sp, other),
    )
    mixcopy.start()

    finish(me_tp)

    weights[0].wait()
    own = mix_ref[pl.ds(pl.multiple_of(me_tp * rows, rows), rows), :]
    own_w = pl.multiple_of(me_tp * half, half)
    oth_w = pl.multiple_of(other * half, half)
    cols = [pl.ds(k * chunk, chunk) for k in range(CHUNKS)]
    part = [dot(own, wo[pl.ds(own_w, half), c]) for c in cols]
    mixcopy.wait_recv()
    peer = mixin[...]
    square = jnp.zeros((rows, 1), jnp.float32)
    for k, c in enumerate(cols):
        total = part[k] + dot(peer, wo[pl.ds(oth_w, half), c])
        summed = (res_ref[:, c].astype(jnp.float32) + total).astype(jnp.bfloat16)
        merged[:, c] = summed
        wide = summed.astype(jnp.float32)
        square = square + jnp.sum(wide * wide, axis=1, keepdims=True)
    inv = lax.rsqrt(square / width + 1e-06)
    for c in cols:
        normed[:, c] = (merged[:, c].astype(jnp.float32) * inv * gain_ref[:, c]).astype(
            jnp.bfloat16
        )

    if lanes > groups * trow:
        pad = lanes - groups * trow
        zrecv[pl.ds(groups * trow, pad), :] = jnp.zeros((pad, width), bf)
    far_rows = lambda g: pl.ds(pl.multiple_of(g * trow, 16), trow)
    near_rows = lambda l: pl.ds(pl.multiple_of(l * TILE, TILE), TILE)
    sends.append(mixcopy)
    order = arrival_order(me_g, groups)

    def home(g):
        return (g * quad + me_q, me_tp)

    early = [pl.ds(0, 2 * narrow)] + [pl.ds((t + 1) * narrow, narrow) for t in range(1, packs)]
    late = [pl.ds(t * narrow, narrow) for t in range(packs - 1)]
    late = late + [pl.ds((packs - 1) * narrow, 2 * narrow)]

    def from_far(i, t):
        there = (far_rows(order[i]), early[t])
        return remote(
            sbuf.at[there], rbuf.at[there], s1.at[0], r1.at[order[i], t], home(order[i])
        )

    sbuf[...] = dot(gather, normed[...]).astype(bf)
    for g in send_order(me_g, groups):
        for t in range(packs):
            remote(
                sbuf.at[far_rows(g), early[t]], rbuf.at[far_rows(me_g), early[t]],
                s1.at[0], r1.at[me_g, t], home(g),
            ).start()
    rbuf[far_rows(me_g), :] = sbuf[far_rows(me_g), :]
    metas.wait_recv()
    out_rows = pl.ds(0, (groups - 1) * trow)
    sends.append(batch(sbuf.at[out_rows], sbuf.at[out_rows], s1.at[0], r1.at[0, 0]))

    slab = GROUP_SIZE * TILE
    parts = [pl.ds(t * narrow, narrow) for t in range(packs)]
    taken = [pl.ds((t + 1) * narrow, narrow) for t in range(packs)]
    lead = pl.ds(0, narrow)
    last = pl.ds(bulk, narrow)

    def keys_of(row, t, p):
        at = row % TILE
        slot = at if t is None else packs * (at - slots) + t
        valid = at < slots if t is None else at >= slots
        if per > 1:
            valid = valid & (slot // cap == p)
        return jnp.where(valid, (row // TILE) * cap + slot - p * cap + 1, -1).astype(jnp.float32)

    down_row = lax.broadcasted_iota(jnp.int32, (slab, trow), 0)
    across_row = lax.broadcasted_iota(jnp.int32, (trow, slab), 1)
    sq_i = lax.broadcasted_iota(jnp.int32, (slab, slab), 0)
    sq_j = lax.broadcasted_iota(jnp.int32, (slab, slab), 1)

    def pairs_of(packed, plain, t):
        same = packed // TILE == plain // TILE
        at = packed % TILE
        hit = same & (at >= slots) & (plain % TILE == packs * (at - slots) + t)
        return jnp.where(hit & (plain % TILE < slots), 1.0, 0.0).astype(bf)

    unpack = [pairs_of(sq_j, sq_i, t) for t in range(packs)]
    repack = [pairs_of(sq_i, sq_j, t) for t in range(packs)]
    plain_row = lax.broadcasted_iota(jnp.int32, (slab, narrow), 0) % TILE < slots

    peers = pl.ds(0, (GROUP_SIZE - 1) * TILE)

    def spread(u, t, src, dst, send, recv):
        for d in range(1, GROUP_SIZE):
            l, dev = near(d)
            remote(
                src.at[u, near_rows(l), parts[t]], dst.at[u, near_rows(me_l), parts[t]],
                send, recv, dev,
            ).start()
        dst[u, near_rows(me_l), parts[t]] = src[u, near_rows(me_l), parts[t]]

    def dispatch(u):
        def pick(p, t):
            table = mrecv[order[u * per + p]][:, 0:trow]
            key = keys_of(down_row, t, p)
            hit = (key == table[0:1, :]) | (key == table[1:2, :])
            return jnp.where(hit, 1.0, 0.0).astype(bf)

        plain = [pick(p, None) for p in range(per)]
        for t in range(packs):
            acc = jnp.zeros((slab, narrow), jnp.float32)
            for p in range(per):
                i = u * per + p
                if i > 0:
                    from_far(i, t).wait_recv()
                acc = acc + dot(plain[p], rbuf[far_rows(order[i]), taken[t]])
                acc = acc + dot(pick(p, t), rbuf[far_rows(order[i]), lead])
            xsend[u, :, parts[t]] = acc.astype(bf)
            spread(u, t, xsend, xin, s2.at[u], r2.at[u])
        sends.append(batch(xsend.at[u, peers], xin.at[u, peers], s2.at[u], r2.at[u]))
        return sends[-1]

    def experts(u, arriving):
        arriving.wait_recv()
        block = xin[u]
        rest = jnp.zeros((slab, narrow), jnp.float32)
        for t in range(packs):
            rest = rest + dot(unpack[t], xin[u, :, parts[t]])
        rest = rest.astype(bf)
        gated = dot(block, wg[narrow:width, :]) + dot(rest, wg[0:narrow, :])
        lifted = dot(block, wu[narrow:width, :]) + dot(rest, wu[0:narrow, :])
        inner = (silu(gated) * lifted).astype(bf)
        ends = dot(inner, wd[:, last]).astype(bf)
        for t in range(packs):
            main = dot(inner, wd[:, parts[t]])
            ysend[u, :, parts[t]] = jnp.where(plain_row, main, dot(repack[t], ends)).astype(bf)

    def give_back(u):
        for t in range(packs):
            spread(u, t, ysend, yrecv, s3.at[u], r3.at[u, t])
        sends.append(batch(ysend.at[u, peers], ysend.at[u, peers], s3.at[u], r3.at[u, 0]))
        return [
            batch(yrecv.at[u, peers, c], yrecv.at[u, peers, c], s3.at[u], r3.at[u, t])
            for t, c in enumerate(parts)
        ]

    def combine(u, arriving):
        def blend(p, t):
            table = mrecv[order[u * per + p]].T[0:trow, :]
            key = keys_of(across_row, t, p)
            both = jnp.where(key == table[:, 0:1], table[:, 2:3], 0.0)
            both = both + jnp.where(key == table[:, 1:2], table[:, 3:4], 0.0)
            high = both.astype(bf)
            return [high, (both - high.astype(jnp.float32)).astype(bf)]

        plain = [blend(p, None) for p in range(per)]
        ends = [jnp.zeros((trow, narrow), jnp.float32) for _ in range(per)]
        for t in range(packs):
            arriving[t].wait_recv()
            for p in range(per):
                i = u * per + p
                mine_z = far_rows(order[i])
                to = zrecv if i == 0 else zsend
                four = dot(jnp.concatenate(plain[p] + blend(p, t), axis=0), yrecv[u, :, parts[t]])
                to[mine_z, parts[t]] = (four[0:trow] + four[trow : 2 * trow]).astype(bf)
                ends[p] = ends[p] + four[2 * trow : 3 * trow] + four[3 * trow : 4 * trow]
                if t == packs - 1:
                    to[mine_z, last] = ends[p].astype(bf)
                if i > 0:
                    remote(
                        zsend.at[mine_z, late[t]], zrecv.at[far_rows(me_g), late[t]],
                        s4.at[0], r4.at[t], home(order[i]),
                    ).start()

    out0 = dispatch(0)
    weights[1].wait()
    weights[2].wait()
    weights[3].wait()
    experts(0, out0)
    out1 = dispatch(1)
    out2 = dispatch(2)
    experts(1, out1)
    out3 = dispatch(3)
    back1 = give_back(1)
    experts(2, out2)
    back2 = give_back(2)
    experts(3, out3)
    back3 = give_back(3)
    back0 = give_back(0)
    combine(1, back1)
    combine(2, back2)
    combine(3, back3)
    combine(0, back0)
    for t, c in enumerate(late):
        batch(zsend.at[out_rows, c], zrecv.at[out_rows, c], s4.at[0], r4.at[t]).wait_recv()
        out_ref[:, c] = (merged[:, c].astype(jnp.float32) + dot(gt, zrecv[:, c])).astype(bf)
    sends.append(batch(zsend.at[out_rows], zsend.at[out_rows], s4.at[0], r4.at[0]))
    for m in sends:
        m.wait_send()


def by_place(me, rows):
    odd, high = me % 2, me // 2
    ones = [(1 - odd) * (1 - high), odd * (1 - high), (1 - odd) * high, odd * high]
    return [sum(one * row[i] for one, row in zip(ones, rows)) for i in range(len(rows[0]))]


def send_order(me, count):
    if count != 4:
        return [lax.rem(me + d, count) for d in range(1, count)]
    return by_place(me, ((3, 1, 2), (3, 2, 0), (0, 1, 3), (0, 2, 1)))


def arrival_order(me, count):
    if count != 4:
        return [me] + [lax.rem(me + count - d, count) for d in range(1, count)]
    return [me] + by_place(me, ((3, 2, 1), (0, 3, 2), (3, 0, 1), (0, 1, 2)))


def rbuf_rows(rows, sp, tp):
    cap = 3 * rows // (sp * tp)
    most = min(GROUP_SIZE * cap // 2, rows)
    return -(-most // 16) * 16


def layer_call(
    q, k, v, og, gl, head_gain, residual, out_weight, norm_gain, routes, group_score, expert_score, wg, wu, wd
):
    sp, tp = lax.axis_size("sp"), lax.axis_size("tp")
    rows, width = residual.shape
    groups = sp * tp // GROUP_SIZE
    cap = 3 * rows // (sp * tp)
    lanes = -(-groups * rbuf_rows(rows, sp, tp) // 128) * 128
    slab = (UNITS, GROUP_SIZE * TILE, width * (groups // UNITS) * cap // TILE)
    quad = GROUP_SIZE // tp
    part = VALUE_DIM // quad
    keys = q.shape[1]
    vm = pl.BlockSpec(memory_space=pltpu.VMEM)
    hb = pl.BlockSpec(memory_space=pl.ANY)
    bf = jnp.bfloat16
    dma = pltpu.SemaphoreType.DMA
    packs = slab[2] // (width - slab[2])
    inputs = (
        gl, k, v, q, routes.T, group_score[None, :], expert_score.T,
        og, head_gain[None, :], residual, norm_gain[None, :],
    )
    return pl.pallas_call(
        functools.partial(layer_kernel, sp, tp),
        out_shape=pltpu.VMEM((rows, width), bf),
        in_specs=[hb] * 15,
        out_specs=vm,
        scratch_shapes=[
            *[pltpu.VMEM(x.shape, x.dtype) for x in inputs],
            pltpu.VMEM(out_weight.shape, bf),
            pltpu.VMEM(wg.shape, bf),
            pltpu.VMEM(wu.shape, bf),
            pltpu.VMEM(wd.shape, bf),
            pltpu.VMEM((rows, v.shape[1]), bf),
            pltpu.VMEM((rows, width), bf),
            pltpu.VMEM((rows, width), bf),
            pltpu.VMEM((lanes, width), bf),
            pltpu.VMEM((lanes, width), bf),
            pltpu.VMEM(slab, bf),
            pltpu.VMEM(slab, bf),
            pltpu.VMEM(slab, bf),
            pltpu.VMEM(slab, bf),
            pltpu.VMEM((lanes, width), bf),
            pltpu.VMEM((lanes, width), bf),
            pltpu.VMEM((groups, 8, 128), jnp.float32),
            pltpu.VMEM((groups, 8, 128), jnp.float32),
            pltpu.VMEM(v.shape, bf),
            pltpu.VMEM(q.shape, bf),
            pltpu.VMEM(v.shape, jnp.float32),
            pltpu.VMEM((quad, part + 16, keys), bf),
            pltpu.VMEM((quad, part + 16, keys), bf),
            pltpu.VMEM((part + 16, keys), bf),
            pltpu.VMEM((groups, part + 16, keys), bf),
            pltpu.VMEM((quad, part, keys), bf),
            pltpu.VMEM((VALUE_DIM, keys), bf),
            dma((1,)), dma((1,)), dma((1,)), dma((1,)), dma((1,)), dma((1,)),
            dma((15,)), dma((2,)), dma((1,)), dma((1,)),
            dma((1,)), dma((groups, packs)), dma((UNITS,)), dma((UNITS,)),
            dma((UNITS,)), dma((UNITS, packs)), dma((1,)), dma((packs,)),
        ],
        compiler_params=pltpu.CompilerParams(
            collective_id=0, has_side_effects=True, vmem_limit_bytes=60 * 1024 * 1024
        ),
    )(*inputs, out_weight, wg, wu, wd)


def local(
    residual,
    queries,
    key_rows,
    value_rows,
    out_gate,
    gate_logits,
    head_gain,
    out_weight,
    norm_gain,
    routes,
    group_score,
    expert_score,
    gate_weight,
    up_weight,
    down_weight,
):
    return layer_call(
        queries, key_rows, value_rows, out_gate, gate_logits, head_gain,
        residual, out_weight, norm_gain, routes, group_score, expert_score,
        gate_weight[0], up_weight[0], down_weight[0],
    )


def solution(mesh):
    placed = (
        P(("sp", "tp"), None),
        P("sp", "tp"),
        P("sp", "tp"),
        P("sp", "tp"),
        P("sp", "tp"),
        P("sp", "tp"),
        P(),
        P(),
        P(),
        P(("sp", "tp"), None),
        P(("sp", "tp")),
        P(("sp", "tp"), None),
        P(("sp", "tp"), None, None),
        P(("sp", "tp"), None, None),
        P(("sp", "tp"), None, None),
    )
    return jax.shard_map(
        local, mesh=mesh, in_specs=placed, out_specs=P(("sp", "tp"), None), check_vma=False
    )
```

```python
import functools

import jax
import jax.numpy as jnp
from jax import lax
from jax.experimental import pallas as pl
from jax.experimental.pallas import tpu as pltpu
from jax.sharding import PartitionSpec as P

KEY_DIM = 64
VALUE_DIM = 128
BLOCK = 64
GROUP_SIZE = 8
MESH = pl.DeviceIdType.MESH
CHUNKS = 4
UNITS = 4
TILE = 16


def dot(a, b):
    return jnp.dot(a, b, preferred_element_type=jnp.float32)


def silu(v):
    return v / (1.0 + jnp.exp(-v))


def layer_kernel(
    sp, tp, gl_hbm, k_hbm, v_hbm, q_hbm, routes_hbm, gscore_hbm, escore_hbm,
    og_hbm, hgain_hbm, res_hbm, gain_hbm, wo_hbm, wg_hbm, wu_hbm, wd_hbm, out_ref,
    gl_ref, k_ref, v_ref, q_ref, routes_ref, gscore_ref, escore_ref,
    og_ref, hgain_ref, res_ref, gain_ref, wo, wg, wu, wd, mixin, merged, normed, sbuf, rbuf, xsend, xin, ysend, yrecv, zsend, zrecv,
    msend, mrecv,
    mix_ref, gather, gated_out, qlead, within, spack, srecv, gpack, grecv, epack, ent,
    ms1, mr1, ms2, mr2, ms3, mr3, isem, mixsem, msem_s, msem_r, s1, r1, s2, r2, s3, r3, s4, r4,
):
    rows, width = res_ref.shape
    half = v_ref.shape[1]
    experts = sp * tp
    cap = 3 * rows // experts
    quad = GROUP_SIZE // tp
    groups = sp // quad
    trow = rbuf_rows(rows, sp, tp)
    per = groups // UNITS
    slots = per * cap
    bulk = width * slots // TILE
    narrow = width - bulk
    packs = bulk // narrow
    lanes = sbuf.shape[0]
    chunk = width // CHUNKS
    me_sp = lax.axis_index("sp")
    me_tp = lax.axis_index("tp")
    me_g = me_sp // quad
    me_q = me_sp % quad
    me_l = me_q * tp + me_tp

    pairs = (
        (gl_hbm, gl_ref), (k_hbm, k_ref), (v_hbm, v_ref), (q_hbm, q_ref),
        (routes_hbm, routes_ref), (gscore_hbm, gscore_ref), (escore_hbm, escore_ref),
        (og_hbm, og_ref), (hgain_hbm, hgain_ref), (res_hbm, res_ref), (gain_hbm, gain_ref),
        (wo_hbm, wo), (wg_hbm, wg), (wu_hbm, wu), (wd_hbm, wd),
    )
    loads = [pltpu.make_async_copy(h, v, isem.at[i]) for i, (h, v) in enumerate(pairs)]
    weights = loads[11:]

    def far(d):
        g = lax.rem(me_g + d, groups)
        return g, (g * quad + me_q, me_tp)

    def near(d):
        l = lax.rem(me_l + d, GROUP_SIZE)
        return l, (me_g * quad + l // tp, l % tp)

    barrier = pltpu.get_barrier_semaphore()
    for d in range(1, groups):
        pl.semaphore_signal(barrier, inc=1, device_id=far(d)[1], device_id_type=MESH)
    for d in range(1, GROUP_SIZE):
        pl.semaphore_signal(barrier, inc=1, device_id=near(d)[1], device_id_type=MESH)
    for w in loads:
        w.start()

    def remote(src, dst, ssem, rsem, dev):
        return pltpu.make_async_remote_copy(
            src_ref=src, dst_ref=dst, send_sem=ssem, recv_sem=rsem, device_id=dev,
            device_id_type=MESH,
        )

    length, keys = q_ref.shape
    heads = keys // KEY_DIM
    blocks = length // BLOCK
    part = VALUE_DIM // quad
    loads[0].wait()
    logits = gl_ref[...].astype(jnp.float32)
    logs = (jnp.minimum(logits, 0.0) - jnp.log1p(jnp.exp(-jnp.abs(logits)))) / 16.0
    pos_i = lax.broadcasted_iota(jnp.int32, (length, length), 0)
    pos_j = lax.broadcasted_iota(jnp.int32, (length, length), 1)
    causal = (pos_i // BLOCK == pos_j // BLOCK) & (pos_j <= pos_i)
    ones = jnp.where(causal, 1.0, 0.0).astype(jnp.bfloat16)
    running = jnp.zeros_like(logs)
    for _ in range(3):
        piece = logs.astype(jnp.bfloat16)
        running = running + dot(ones, piece)
        logs = logs - piece.astype(jnp.float32)
    split = [slice(n * BLOCK, (n + 1) * BLOCK) for n in range(blocks)]
    closing = [running[(n + 1) * BLOCK - 1 : (n + 1) * BLOCK, :] for n in range(blocks)]
    loads[1].wait()
    key_float = k_ref[...].astype(jnp.float32)
    key_closing = [key_float[s] * jnp.exp(closing[n] - running[s]) for n, s in enumerate(split)]
    key_end = list(key_closing)
    tail = jnp.zeros_like(closing[0])
    for n in range(blocks - 1, -1, -1):
        if n < blocks - 1:
            key_end[n] = key_closing[n] * jnp.exp(tail)
        tail = tail + closing[n]
    key_end = jnp.concatenate(key_end, axis=0).astype(jnp.bfloat16)
    low = lax.broadcasted_iota(jnp.int32, (VALUE_DIM, 2 * KEY_DIM), 1) < KEY_DIM
    bf = jnp.bfloat16
    tile = lax.broadcasted_iota(jnp.int32, (16, keys), 0)

    def as_rows(factor):
        high = factor.astype(bf).astype(jnp.float32)
        return jnp.where(tile == 0, high, jnp.where(tile == 1, factor - high, 0.0)).astype(bf)

    def factor_of(rows16):
        wide = rows16.astype(jnp.float32)
        return wide[0:1] + wide[1:2]

    loads[2].wait()
    for p in range(heads // 2):
        pair = slice(p * 2 * KEY_DIM, (p + 1) * 2 * KEY_DIM)
        both = [
            lax.dot_general(
                v_ref[:, h * VALUE_DIM : (h + 1) * VALUE_DIM], key_end[:, pair],
                (((0,), (0,)), ((), ())), preferred_element_type=jnp.float32,
            )
            for h in (2 * p, 2 * p + 1)
        ]
        end = jnp.where(low, both[0], both[1])
        for j in range(quad):
            spack[j, 0:part, pair] = end[j * part : (j + 1) * part].astype(bf)
    decay_rows = as_rows(jnp.exp(tail))
    for j in range(quad):
        spack[j, part : part + 16, :] = decay_rows
    pl.semaphore_wait(barrier, groups - 1 + GROUP_SIZE - 1)

    def side(d):
        j = lax.rem(me_q + d, quad)
        return j, (me_g * quad + j, me_tp)

    beside = side(1)[1]

    def batch(src, dst, ss, rr):
        return remote(src, dst, ss, rr, beside)

    for d in range(1, quad):
        j, dev = side(d)
        remote(spack.at[j], srecv.at[me_q], ms1.at[0], mr1.at[0], dev).start()
    others = pl.ds(0, quad - 1)
    hop1 = batch(spack.at[others], srecv.at[others], ms1.at[0], mr1.at[0])
    srecv[me_q] = spack[me_q]

    loads[3].wait()
    query = q_ref[...].astype(jnp.float32) * KEY_DIM ** (-0.5) * jnp.exp(running)
    key_inverse = (key_float * jnp.exp(-running)).astype(jnp.bfloat16)
    query_bf = query.astype(jnp.bfloat16)
    lead = jnp.zeros_like(closing[0])
    for n, s in enumerate(split):
        qlead[s, :] = (query[s] * jnp.exp(lead)).astype(jnp.bfloat16)
        lead = lead + closing[n]
    older = []
    for n in range(1, blocks):
        pieces = []
        gap = jnp.zeros_like(closing[0])
        for m in range(n - 1, -1, -1):
            pieces.insert(0, key_closing[m] if m == n - 1 else key_closing[m] * jnp.exp(gap))
            gap = gap + closing[m]
        pieces.append(jnp.zeros((length - n * BLOCK, keys), jnp.float32))
        older.append(jnp.concatenate(pieces, axis=0).astype(jnp.bfloat16))
    lane2 = lax.broadcasted_iota(jnp.int32, (length, 2 * KEY_DIM), 1)
    nt = (((1,), (1,)), ((), ()))

    def of_head(x, h):
        keep = lane2[: x.shape[0]] < KEY_DIM if h % 2 == 0 else lane2[: x.shape[0]] >= KEY_DIM
        return jnp.where(keep, x, jnp.zeros_like(x))

    for h in range(heads):
        pair = slice(h // 2 * 2 * KEY_DIM, (h // 2 + 1) * 2 * KEY_DIM)
        mine_q = of_head(query_bf[:, pair], h)
        score = lax.dot_general(
            mine_q, key_inverse[:, pair], nt, preferred_element_type=jnp.float32
        )
        past = [jnp.zeros((BLOCK, length), jnp.float32)]
        for n in range(1, blocks):
            past.append(
                lax.dot_general(
                    mine_q[split[n]], older[n - 1][:, pair], nt,
                    preferred_element_type=jnp.float32,
                )
            )
        score = jnp.where(causal, score, jnp.concatenate(past, axis=0)).astype(jnp.bfloat16)
        hv = slice(h * VALUE_DIM, (h + 1) * VALUE_DIM)
        within[:, hv] = dot(score, v_ref[:, hv])

    hop1.wait_recv()
    total = jnp.zeros((part, keys), jnp.float32)
    total_decay = jnp.ones((1, keys), jnp.float32)
    before_state, before_decay = [], []
    for j in range(quad):
        before_state.append(total)
        before_decay.append(total_decay)
        step = factor_of(srecv[j, part : part + 16, :])
        total = step * total + srecv[j, 0:part, :].astype(jnp.float32)
        total_decay = total_decay * step
    gpack[0:part, :] = total.astype(bf)
    gpack[part : part + 16, :] = as_rows(total_decay)
    for d in range(1, groups):
        g, dev = far(d)
        remote(gpack, grecv.at[me_g], ms2.at[0], mr2.at[0], dev).start()
    apart = pl.ds(0, groups - 1)
    hop2 = batch(grecv.at[apart], grecv.at[apart], ms2.at[0], mr2.at[0])
    grecv[me_g] = gpack[...]

    for w in loads[4:11]:
        w.wait()
    sub = lax.broadcasted_iota(jnp.int32, (rows, rows), 0)
    route_t = routes_ref[...].astype(jnp.float32)
    score_t = escore_ref[...]
    scale_t = gscore_ref[...] * score_t / jnp.sum(score_t, axis=0, keepdims=True)
    columns = jnp.where(sub == 0, route_t[0:1, :], 0.0) + jnp.where(sub == 1, route_t[1:2, :], 0.0)
    columns = columns.T
    ra = columns[:, 0:1].astype(jnp.int32)
    rb = columns[:, 1:2].astype(jnp.int32)
    elane = lax.broadcasted_iota(jnp.int32, (rows, 128), 1)
    row_i = lax.broadcasted_iota(jnp.int32, (rows, rows), 0)
    col_i = lax.broadcasted_iota(jnp.int32, (rows, rows), 1)
    strict = jnp.where(col_i < row_i, 1.0, 0.0).astype(jnp.bfloat16)
    is_a = elane == ra
    is_b = elane == rb
    either = (jnp.where(is_a, 1.0, 0.0) + jnp.where(is_b, 1.0, 0.0)).astype(jnp.bfloat16)
    before = dot(strict, either)
    rank_a = jnp.sum(jnp.where(is_a, before, 0.0), axis=1, keepdims=True)
    rank_b = jnp.sum(jnp.where(is_b, before, 0.0), axis=1, keepdims=True)
    group = ra // GROUP_SIZE
    is_g = elane == group
    before_g = dot(strict, jnp.where(is_g, 1.0, 0.0).astype(jnp.bfloat16))
    rank_g = jnp.sum(jnp.where(is_g, before_g, 0.0), axis=1, keepdims=True).astype(jnp.int32)
    code_a = ((ra % GROUP_SIZE) * cap + 1).astype(jnp.float32) + rank_a
    code_b = ((rb % GROUP_SIZE) * cap + 1).astype(jnp.float32) + rank_b
    values = jnp.where(elane == 0, code_a, 0.0) + jnp.where(elane == 1, code_b, 0.0)
    values_t = values.T[0:8, :]
    sub8 = lax.broadcasted_iota(jnp.int32, (8, rows), 0)
    values_t = values_t + jnp.where(sub8 == 2, scale_t[0:1, :], 0.0)
    values_t = values_t + jnp.where(sub8 == 3, scale_t[1:2, :], 0.0)
    slot_lane = lax.broadcasted_iota(jnp.int32, (rows, lanes), 1)
    mine = jnp.where(elane == rank_g, 1.0, 0.0)
    for g in range(groups):
        msend[g] = jnp.dot(
            values_t, jnp.where(group == g, mine, 0.0),
            preferred_element_type=jnp.float32, precision=lax.Precision.HIGHEST,
        )
    mrecv[me_g] = msend[me_g]
    for d in range(1, groups):
        g, dev = far(d)
        remote(msend.at[g], mrecv.at[me_g], msem_s.at[0], msem_r.at[0], dev).start()
    metas = batch(msend.at[apart], mrecv.at[apart], msem_s.at[0], msem_r.at[0])
    gt = jnp.where(slot_lane == group * trow + rank_g, 1.0, 0.0)
    gather[...] = gt.T.astype(jnp.bfloat16)
    gt = gt.astype(jnp.bfloat16)
    for h in range(heads):
        hv = slice(h * VALUE_DIM, (h + 1) * VALUE_DIM)
        gated_out[:, hv] = hgain_ref[...] * silu(og_ref[:, hv].astype(jnp.float32))

    hop2.wait_recv()
    state = jnp.zeros((part, keys), jnp.float32)
    for g in range(groups - 1):
        step = factor_of(grecv[g, part : part + 16, :])
        state = jnp.where(me_g > g, step * state + grecv[g, 0:part, :].astype(jnp.float32), state)
    for j in range(quad):
        epack[j] = (before_decay[j] * state + before_state[j]).astype(jnp.bfloat16)
    mine_v = pl.ds(pl.multiple_of(me_q * part, part), part)
    for d in range(1, quad):
        j, dev = side(d)
        remote(epack.at[j], ent.at[mine_v], ms3.at[0], mr3.at[0], dev).start()
    ent[mine_v, :] = epack[me_q]
    slices = pl.ds(0, (quad - 1) * part)
    hop3 = batch(ent.at[slices], ent.at[slices], ms3.at[0], mr3.at[0])
    hop3.wait_recv()
    sends = [hop1, hop2, hop3, metas]
    entering = ent[...]

    def finish(which):
        at = pl.ds(pl.multiple_of(which * rows, rows), rows)
        for h in range(heads):
            pair = slice(h // 2 * 2 * KEY_DIM, (h // 2 + 1) * 2 * KEY_DIM)
            hv = slice(h * VALUE_DIM, (h + 1) * VALUE_DIM)
            attended = within[at, hv] + lax.dot_general(
                of_head(qlead[at, pair], h), entering[:, pair], nt,
                preferred_element_type=jnp.float32,
            )
            mean = jnp.mean(attended * attended, axis=1, keepdims=True)
            unit = attended * lax.rsqrt(mean + 1e-06)
            mix_ref[at, hv] = (unit * gated_out[at, hv]).astype(jnp.bfloat16)

    other = 1 - me_tp
    finish(other)
    mixcopy = remote(
        mix_ref.at[pl.ds(pl.multiple_of(other * rows, rows), rows)], mixin,
        mixsem.at[0], mixsem.at[1], (me_sp, other),
    )
    mixcopy.start()

    finish(me_tp)

    weights[0].wait()
    own = mix_ref[pl.ds(pl.multiple_of(me_tp * rows, rows), rows), :]
    own_w = pl.multiple_of(me_tp * half, half)
    oth_w = pl.multiple_of(other * half, half)
    cols = [pl.ds(k * chunk, chunk) for k in range(CHUNKS)]
    part = [dot(own, wo[pl.ds(own_w, half), c]) for c in cols]
    mixcopy.wait_recv()
    peer = mixin[...]
    square = jnp.zeros((rows, 1), jnp.float32)
    for k, c in enumerate(cols):
        total = part[k] + dot(peer, wo[pl.ds(oth_w, half), c])
        summed = (res_ref[:, c].astype(jnp.float32) + total).astype(jnp.bfloat16)
        merged[:, c] = summed
        wide = summed.astype(jnp.float32)
        square = square + jnp.sum(wide * wide, axis=1, keepdims=True)
    inv = lax.rsqrt(square / width + 1e-06)
    for c in cols:
        normed[:, c] = (merged[:, c].astype(jnp.float32) * inv * gain_ref[:, c]).astype(
            jnp.bfloat16
        )

    if lanes > groups * trow:
        pad = lanes - groups * trow
        zrecv[pl.ds(groups * trow, pad), :] = jnp.zeros((pad, width), bf)
    far_rows = lambda g: pl.ds(pl.multiple_of(g * trow, 16), trow)
    near_rows = lambda l: pl.ds(pl.multiple_of(l * TILE, TILE), TILE)
    sends.append(mixcopy)
    order = arrival_order(me_g, groups)

    def home(g):
        return (g * quad + me_q, me_tp)

    early = [pl.ds(0, 2 * narrow)] + [pl.ds((t + 1) * narrow, narrow) for t in range(1, packs)]
    late = [pl.ds(t * narrow, narrow) for t in range(packs - 1)]
    late = late + [pl.ds((packs - 1) * narrow, 2 * narrow)]

    def from_far(i, t):
        there = (far_rows(order[i]), early[t])
        return remote(
            sbuf.at[there], rbuf.at[there], s1.at[0], r1.at[order[i], t], home(order[i])
        )

    ready = normed[...]
    for g in send_order(me_g, groups):
        sbuf[far_rows(g), :] = dot(gather[far_rows(g), :], ready).astype(bf)
        for t in range(packs):
            remote(
                sbuf.at[far_rows(g), early[t]], rbuf.at[far_rows(me_g), early[t]],
                s1.at[0], r1.at[me_g, t], home(g),
            ).start()
    rbuf[far_rows(me_g), :] = dot(gather[far_rows(me_g), :], ready).astype(bf)
    metas.wait_recv()
    out_rows = pl.ds(0, (groups - 1) * trow)
    sends.append(batch(sbuf.at[out_rows], sbuf.at[out_rows], s1.at[0], r1.at[0, 0]))

    slab = GROUP_SIZE * TILE
    parts = [pl.ds(t * narrow, narrow) for t in range(packs)]
    taken = [pl.ds((t + 1) * narrow, narrow) for t in range(packs)]
    lead = pl.ds(0, narrow)
    last = pl.ds(bulk, narrow)

    def keys_of(row, t, p):
        at = row % TILE
        slot = at if t is None else packs * (at - slots) + t
        valid = at < slots if t is None else at >= slots
        if per > 1:
            valid = valid & (slot // cap == p)
        return jnp.where(valid, (row // TILE) * cap + slot - p * cap + 1, -1).astype(jnp.float32)

    down_row = lax.broadcasted_iota(jnp.int32, (slab, trow), 0)
    across_row = lax.broadcasted_iota(jnp.int32, (trow, slab), 1)
    sq_i = lax.broadcasted_iota(jnp.int32, (slab, slab), 0)
    sq_j = lax.broadcasted_iota(jnp.int32, (slab, slab), 1)

    def pairs_of(packed, plain, t):
        same = packed // TILE == plain // TILE
        at = packed % TILE
        hit = same & (at >= slots) & (plain % TILE == packs * (at - slots) + t)
        return jnp.where(hit & (plain % TILE < slots), 1.0, 0.0).astype(bf)

    unpack = [pairs_of(sq_j, sq_i, t) for t in range(packs)]
    repack = [pairs_of(sq_i, sq_j, t) for t in range(packs)]
    plain_row = lax.broadcasted_iota(jnp.int32, (slab, narrow), 0) % TILE < slots

    peers = pl.ds(0, (GROUP_SIZE - 1) * TILE)

    def spread(u, t, src, dst, send, recv):
        for d in range(1, GROUP_SIZE):
            l, dev = near(d)
            remote(
                src.at[u, near_rows(l), parts[t]], dst.at[u, near_rows(me_l), parts[t]],
                send, recv, dev,
            ).start()
        dst[u, near_rows(me_l), parts[t]] = src[u, near_rows(me_l), parts[t]]

    def dispatch(u):
        def pick(p, t):
            table = mrecv[order[u * per + p]][:, 0:trow]
            key = keys_of(down_row, t, p)
            hit = (key == table[0:1, :]) | (key == table[1:2, :])
            return jnp.where(hit, 1.0, 0.0).astype(bf)

        plain = [pick(p, None) for p in range(per)]
        for t in range(packs):
            acc = jnp.zeros((slab, narrow), jnp.float32)
            for p in range(per):
                i = u * per + p
                if i > 0:
                    from_far(i, t).wait_recv()
                acc = acc + dot(plain[p], rbuf[far_rows(order[i]), taken[t]])
                acc = acc + dot(pick(p, t), rbuf[far_rows(order[i]), lead])
            xsend[u, :, parts[t]] = acc.astype(bf)
            spread(u, t, xsend, xin, s2.at[u], r2.at[u])
        sends.append(batch(xsend.at[u, peers], xin.at[u, peers], s2.at[u], r2.at[u]))
        return sends[-1]

    def experts(u, arriving):
        arriving.wait_recv()
        block = xin[u]
        rest = jnp.zeros((slab, narrow), jnp.float32)
        for t in range(packs):
            rest = rest + dot(unpack[t], xin[u, :, parts[t]])
        rest = rest.astype(bf)
        gated = dot(block, wg[narrow:width, :]) + dot(rest, wg[0:narrow, :])
        lifted = dot(block, wu[narrow:width, :]) + dot(rest, wu[0:narrow, :])
        inner = (silu(gated) * lifted).astype(bf)
        ends = dot(inner, wd[:, last]).astype(bf)
        for t in range(packs):
            main = dot(inner, wd[:, parts[t]])
            ysend[u, :, parts[t]] = jnp.where(plain_row, main, dot(repack[t], ends)).astype(bf)

    def give_back(u):
        for t in range(packs):
            spread(u, t, ysend, yrecv, s3.at[u], r3.at[u, t])
        sends.append(batch(ysend.at[u, peers], ysend.at[u, peers], s3.at[u], r3.at[u, 0]))
        return [
            batch(yrecv.at[u, peers, c], yrecv.at[u, peers, c], s3.at[u], r3.at[u, t])
            for t, c in enumerate(parts)
        ]

    def combine(u, arriving):
        def blend(p, t):
            table = mrecv[order[u * per + p]].T[0:trow, :]
            key = keys_of(across_row, t, p)
            both = jnp.where(key == table[:, 0:1], table[:, 2:3], 0.0)
            both = both + jnp.where(key == table[:, 1:2], table[:, 3:4], 0.0)
            high = both.astype(bf)
            return [high, (both - high.astype(jnp.float32)).astype(bf)]

        plain = [blend(p, None) for p in range(per)]
        ends = [jnp.zeros((trow, narrow), jnp.float32) for _ in range(per)]
        for t in range(packs):
            arriving[t].wait_recv()
            for p in range(per):
                i = u * per + p
                mine_z = far_rows(order[i])
                to = zrecv if i == 0 else zsend
                four = dot(jnp.concatenate(plain[p] + blend(p, t), axis=0), yrecv[u, :, parts[t]])
                to[mine_z, parts[t]] = (four[0:trow] + four[trow : 2 * trow]).astype(bf)
                ends[p] = ends[p] + four[2 * trow : 3 * trow] + four[3 * trow : 4 * trow]
                if t == packs - 1:
                    to[mine_z, last] = ends[p].astype(bf)
                if i > 0:
                    remote(
                        zsend.at[mine_z, late[t]], zrecv.at[far_rows(me_g), late[t]],
                        s4.at[0], r4.at[t], home(order[i]),
                    ).start()

    out0 = dispatch(0)
    weights[1].wait()
    weights[2].wait()
    weights[3].wait()
    out1 = dispatch(1)
    experts(0, out0)
    out2 = dispatch(2)
    experts(1, out1)
    back1 = give_back(1)
    out3 = dispatch(3)
    experts(2, out2)
    back2 = give_back(2)
    combine(1, back1)
    experts(3, out3)
    back3 = give_back(3)
    back0 = give_back(0)
    combine(2, back2)
    combine(3, back3)
    combine(0, back0)
    for t, c in enumerate(late):
        batch(zsend.at[out_rows, c], zrecv.at[out_rows, c], s4.at[0], r4.at[t]).wait_recv()
        out_ref[:, c] = (merged[:, c].astype(jnp.float32) + dot(gt, zrecv[:, c])).astype(bf)
    sends.append(batch(zsend.at[out_rows], zsend.at[out_rows], s4.at[0], r4.at[0]))
    for m in sends:
        m.wait_send()


def by_place(me, rows):
    odd, high = me % 2, me // 2
    ones = [(1 - odd) * (1 - high), odd * (1 - high), (1 - odd) * high, odd * high]
    return [sum(one * row[i] for one, row in zip(ones, rows)) for i in range(len(rows[0]))]


def send_order(me, count):
    if count != 4:
        return [lax.rem(me + d, count) for d in range(1, count)]
    return by_place(me, ((3, 1, 2), (3, 2, 0), (0, 1, 3), (0, 2, 1)))


def arrival_order(me, count):
    if count != 4:
        return [me] + [lax.rem(me + count - d, count) for d in range(1, count)]
    return [me] + by_place(me, ((3, 2, 1), (0, 3, 2), (3, 0, 1), (0, 1, 2)))


def rbuf_rows(rows, sp, tp):
    cap = 3 * rows // (sp * tp)
    most = min(GROUP_SIZE * cap // 2, rows)
    return -(-most // 16) * 16


def layer_call(
    q, k, v, og, gl, head_gain, residual, out_weight, norm_gain, routes, group_score, expert_score, wg, wu, wd
):
    sp, tp = lax.axis_size("sp"), lax.axis_size("tp")
    rows, width = residual.shape
    groups = sp * tp // GROUP_SIZE
    cap = 3 * rows // (sp * tp)
    lanes = -(-groups * rbuf_rows(rows, sp, tp) // 128) * 128
    slab = (UNITS, GROUP_SIZE * TILE, width * (groups // UNITS) * cap // TILE)
    quad = GROUP_SIZE // tp
    part = VALUE_DIM // quad
    keys = q.shape[1]
    vm = pl.BlockSpec(memory_space=pltpu.VMEM)
    hb = pl.BlockSpec(memory_space=pl.ANY)
    bf = jnp.bfloat16
    dma = pltpu.SemaphoreType.DMA
    packs = slab[2] // (width - slab[2])
    inputs = (
        gl, k, v, q, routes.T, group_score[None, :], expert_score.T,
        og, head_gain[None, :], residual, norm_gain[None, :],
    )
    return pl.pallas_call(
        functools.partial(layer_kernel, sp, tp),
        out_shape=pltpu.VMEM((rows, width), bf),
        in_specs=[hb] * 15,
        out_specs=vm,
        scratch_shapes=[
            *[pltpu.VMEM(x.shape, x.dtype) for x in inputs],
            pltpu.VMEM(out_weight.shape, bf),
            pltpu.VMEM(wg.shape, bf),
            pltpu.VMEM(wu.shape, bf),
            pltpu.VMEM(wd.shape, bf),
            pltpu.VMEM((rows, v.shape[1]), bf),
            pltpu.VMEM((rows, width), bf),
            pltpu.VMEM((rows, width), bf),
            pltpu.VMEM((lanes, width), bf),
            pltpu.VMEM((lanes, width), bf),
            pltpu.VMEM(slab, bf),
            pltpu.VMEM(slab, bf),
            pltpu.VMEM(slab, bf),
            pltpu.VMEM(slab, bf),
            pltpu.VMEM((lanes, width), bf),
            pltpu.VMEM((lanes, width), bf),
            pltpu.VMEM((groups, 8, 128), jnp.float32),
            pltpu.VMEM((groups, 8, 128), jnp.float32),
            pltpu.VMEM(v.shape, bf),
            pltpu.VMEM((lanes, rows), bf),
            pltpu.VMEM(v.shape, jnp.float32),
            pltpu.VMEM(q.shape, bf),
            pltpu.VMEM(v.shape, jnp.float32),
            pltpu.VMEM((quad, part + 16, keys), bf),
            pltpu.VMEM((quad, part + 16, keys), bf),
            pltpu.VMEM((part + 16, keys), bf),
            pltpu.VMEM((groups, part + 16, keys), bf),
            pltpu.VMEM((quad, part, keys), bf),
            pltpu.VMEM((VALUE_DIM, keys), bf),
            dma((1,)), dma((1,)), dma((1,)), dma((1,)), dma((1,)), dma((1,)),
            dma((15,)), dma((2,)), dma((1,)), dma((1,)),
            dma((1,)), dma((groups, packs)), dma((UNITS,)), dma((UNITS,)),
            dma((UNITS,)), dma((UNITS, packs)), dma((1,)), dma((packs,)),
        ],
        compiler_params=pltpu.CompilerParams(
            collective_id=0, has_side_effects=True, vmem_limit_bytes=60 * 1024 * 1024
        ),
    )(*inputs, out_weight, wg, wu, wd)


def local(
    residual,
    queries,
    key_rows,
    value_rows,
    out_gate,
    gate_logits,
    head_gain,
    out_weight,
    norm_gain,
    routes,
    group_score,
    expert_score,
    gate_weight,
    up_weight,
    down_weight,
):
    return layer_call(
        queries, key_rows, value_rows, out_gate, gate_logits, head_gain,
        residual, out_weight, norm_gain, routes, group_score, expert_score,
        gate_weight[0], up_weight[0], down_weight[0],
    )


def solution(mesh):
    placed = (
        P(("sp", "tp"), None),
        P("sp", "tp"),
        P("sp", "tp"),
        P("sp", "tp"),
        P("sp", "tp"),
        P("sp", "tp"),
        P(),
        P(),
        P(),
        P(("sp", "tp"), None),
        P(("sp", "tp")),
        P(("sp", "tp"), None),
        P(("sp", "tp"), None, None),
        P(("sp", "tp"), None, None),
        P(("sp", "tp"), None, None),
    )
    return jax.shard_map(
        local, mesh=mesh, in_specs=placed, out_specs=P(("sp", "tp"), None), check_vma=False
    )
```

```python
import functools

import jax
import jax.numpy as jnp
from jax import lax
from jax.experimental import pallas as pl
from jax.experimental.pallas import tpu as pltpu
from jax.sharding import PartitionSpec as P

KEY_DIM = 64
VALUE_DIM = 128
BLOCK = 64
GROUP_SIZE = 8
MESH = pl.DeviceIdType.MESH
CHUNKS = 4
UNITS = 4
TILE = 16


def dot(a, b):
    return jnp.dot(a, b, preferred_element_type=jnp.float32)


def silu(v):
    return v / (1.0 + jnp.exp(-v))


def layer_kernel(
    sp, tp, gl_hbm, k_hbm, v_hbm, q_hbm, routes_hbm, gscore_hbm, escore_hbm,
    og_hbm, hgain_hbm, res_hbm, gain_hbm, wo_hbm, wg_hbm, wu_hbm, wd_hbm, out_ref,
    gl_ref, k_ref, v_ref, q_ref, routes_ref, gscore_ref, escore_ref,
    og_ref, hgain_ref, res_ref, gain_ref, wo, wg, wu, wd, mixin, merged, normed, sbuf, rbuf, xsend, xin, ysend, yrecv, zsend, zrecv,
    msend, mrecv,
    mix_ref, gather, gated_out, qlead, within, spack, srecv, gpack, grecv, epack, ent,
    ms1, mr1, ms2, mr2, ms3, mr3, isem, mixsem, msem_s, msem_r, s1, r1, s2, r2, s3, r3, s4, r4,
):
    rows, width = res_ref.shape
    half = v_ref.shape[1]
    experts = sp * tp
    cap = 3 * rows // experts
    quad = GROUP_SIZE // tp
    groups = sp // quad
    trow = rbuf_rows(rows, sp, tp)
    per = groups // UNITS
    slots = per * cap
    bulk = width * slots // TILE
    narrow = width - bulk
    packs = bulk // narrow
    lanes = sbuf.shape[0]
    chunk = width // CHUNKS
    me_sp = lax.axis_index("sp")
    me_tp = lax.axis_index("tp")
    me_g = me_sp // quad
    me_q = me_sp % quad
    me_l = me_q * tp + me_tp

    pairs = (
        (gl_hbm, gl_ref), (k_hbm, k_ref), (v_hbm, v_ref), (q_hbm, q_ref),
        (routes_hbm, routes_ref), (gscore_hbm, gscore_ref), (escore_hbm, escore_ref),
        (og_hbm, og_ref), (hgain_hbm, hgain_ref), (res_hbm, res_ref), (gain_hbm, gain_ref),
        (wo_hbm, wo), (wg_hbm, wg), (wu_hbm, wu), (wd_hbm, wd),
    )
    loads = [pltpu.make_async_copy(h, v, isem.at[i]) for i, (h, v) in enumerate(pairs)]
    weights = loads[11:]

    def far(d):
        g = lax.rem(me_g + d, groups)
        return g, (g * quad + me_q, me_tp)

    def near(d):
        l = lax.rem(me_l + d, GROUP_SIZE)
        return l, (me_g * quad + l // tp, l % tp)

    barrier = pltpu.get_barrier_semaphore()
    for d in range(1, groups):
        pl.semaphore_signal(barrier, inc=1, device_id=far(d)[1], device_id_type=MESH)
    for d in range(1, GROUP_SIZE):
        pl.semaphore_signal(barrier, inc=1, device_id=near(d)[1], device_id_type=MESH)
    for w in loads:
        w.start()

    def remote(src, dst, ssem, rsem, dev):
        return pltpu.make_async_remote_copy(
            src_ref=src, dst_ref=dst, send_sem=ssem, recv_sem=rsem, device_id=dev,
            device_id_type=MESH,
        )

    length, keys = q_ref.shape
    heads = keys // KEY_DIM
    blocks = length // BLOCK
    part = VALUE_DIM // quad
    loads[0].wait()
    logits = gl_ref[...].astype(jnp.float32)
    logs = (jnp.minimum(logits, 0.0) - jnp.log1p(jnp.exp(-jnp.abs(logits)))) / 16.0
    pos_i = lax.broadcasted_iota(jnp.int32, (length, length), 0)
    pos_j = lax.broadcasted_iota(jnp.int32, (length, length), 1)
    causal = (pos_i // BLOCK == pos_j // BLOCK) & (pos_j <= pos_i)
    ones = jnp.where(causal, 1.0, 0.0).astype(jnp.bfloat16)
    running = jnp.zeros_like(logs)
    for _ in range(3):
        piece = logs.astype(jnp.bfloat16)
        running = running + dot(ones, piece)
        logs = logs - piece.astype(jnp.float32)
    split = [slice(n * BLOCK, (n + 1) * BLOCK) for n in range(blocks)]
    closing = [running[(n + 1) * BLOCK - 1 : (n + 1) * BLOCK, :] for n in range(blocks)]
    loads[1].wait()
    key_float = k_ref[...].astype(jnp.float32)
    key_closing = [key_float[s] * jnp.exp(closing[n] - running[s]) for n, s in enumerate(split)]
    key_end = list(key_closing)
    tail = jnp.zeros_like(closing[0])
    for n in range(blocks - 1, -1, -1):
        if n < blocks - 1:
            key_end[n] = key_closing[n] * jnp.exp(tail)
        tail = tail + closing[n]
    key_end = jnp.concatenate(key_end, axis=0).astype(jnp.bfloat16)
    low = lax.broadcasted_iota(jnp.int32, (VALUE_DIM, 2 * KEY_DIM), 1) < KEY_DIM
    bf = jnp.bfloat16
    tile = lax.broadcasted_iota(jnp.int32, (16, keys), 0)

    def as_rows(factor):
        high = factor.astype(bf).astype(jnp.float32)
        return jnp.where(tile == 0, high, jnp.where(tile == 1, factor - high, 0.0)).astype(bf)

    def factor_of(rows16):
        wide = rows16.astype(jnp.float32)
        return wide[0:1] + wide[1:2]

    loads[2].wait()
    for p in range(heads // 2):
        pair = slice(p * 2 * KEY_DIM, (p + 1) * 2 * KEY_DIM)
        both = [
            lax.dot_general(
                v_ref[:, h * VALUE_DIM : (h + 1) * VALUE_DIM], key_end[:, pair],
                (((0,), (0,)), ((), ())), preferred_element_type=jnp.float32,
            )
            for h in (2 * p, 2 * p + 1)
        ]
        end = jnp.where(low, both[0], both[1])
        for j in range(quad):
            spack[j, 0:part, pair] = end[j * part : (j + 1) * part].astype(bf)
    decay_rows = as_rows(jnp.exp(tail))
    for j in range(quad):
        spack[j, part : part + 16, :] = decay_rows
    pl.semaphore_wait(barrier, groups - 1 + GROUP_SIZE - 1)

    def side(d):
        j = lax.rem(me_q + d, quad)
        return j, (me_g * quad + j, me_tp)

    beside = side(1)[1]

    def batch(src, dst, ss, rr):
        return remote(src, dst, ss, rr, beside)

    for d in range(1, quad):
        j, dev = side(d)
        remote(spack.at[j], srecv.at[me_q], ms1.at[0], mr1.at[0], dev).start()
    others = pl.ds(0, quad - 1)
    hop1 = batch(spack.at[others], srecv.at[others], ms1.at[0], mr1.at[0])
    srecv[me_q] = spack[me_q]

    loads[3].wait()
    query = q_ref[...].astype(jnp.float32) * KEY_DIM ** (-0.5) * jnp.exp(running)
    key_inverse = (key_float * jnp.exp(-running)).astype(jnp.bfloat16)
    query_bf = query.astype(jnp.bfloat16)
    lead = jnp.zeros_like(closing[0])
    for n, s in enumerate(split):
        qlead[s, :] = (query[s] * jnp.exp(lead)).astype(jnp.bfloat16)
        lead = lead + closing[n]
    older = []
    for n in range(1, blocks):
        pieces = []
        gap = jnp.zeros_like(closing[0])
        for m in range(n - 1, -1, -1):
            pieces.insert(0, key_closing[m] if m == n - 1 else key_closing[m] * jnp.exp(gap))
            gap = gap + closing[m]
        pieces.append(jnp.zeros((length - n * BLOCK, keys), jnp.float32))
        older.append(jnp.concatenate(pieces, axis=0).astype(jnp.bfloat16))
    lane2 = lax.broadcasted_iota(jnp.int32, (length, 2 * KEY_DIM), 1)
    nt = (((1,), (1,)), ((), ()))

    def of_head(x, h):
        keep = lane2[: x.shape[0]] < KEY_DIM if h % 2 == 0 else lane2[: x.shape[0]] >= KEY_DIM
        return jnp.where(keep, x, jnp.zeros_like(x))

    for h in range(heads):
        pair = slice(h // 2 * 2 * KEY_DIM, (h // 2 + 1) * 2 * KEY_DIM)
        mine_q = of_head(query_bf[:, pair], h)
        score = lax.dot_general(
            mine_q, key_inverse[:, pair], nt, preferred_element_type=jnp.float32
        )
        past = [jnp.zeros((BLOCK, length), jnp.float32)]
        for n in range(1, blocks):
            past.append(
                lax.dot_general(
                    mine_q[split[n]], older[n - 1][:, pair], nt,
                    preferred_element_type=jnp.float32,
                )
            )
        score = jnp.where(causal, score, jnp.concatenate(past, axis=0)).astype(jnp.bfloat16)
        hv = slice(h * VALUE_DIM, (h + 1) * VALUE_DIM)
        within[:, hv] = dot(score, v_ref[:, hv])

    hop1.wait_recv()
    total = jnp.zeros((part, keys), jnp.float32)
    total_decay = jnp.ones((1, keys), jnp.float32)
    before_state, before_decay = [], []
    for j in range(quad):
        before_state.append(total)
        before_decay.append(total_decay)
        step = factor_of(srecv[j, part : part + 16, :])
        total = step * total + srecv[j, 0:part, :].astype(jnp.float32)
        total_decay = total_decay * step
    gpack[0:part, :] = total.astype(bf)
    gpack[part : part + 16, :] = as_rows(total_decay)
    for d in range(1, groups):
        g, dev = far(d)
        remote(gpack, grecv.at[me_g], ms2.at[0], mr2.at[0], dev).start()
    apart = pl.ds(0, groups - 1)
    hop2 = batch(grecv.at[apart], grecv.at[apart], ms2.at[0], mr2.at[0])
    grecv[me_g] = gpack[...]

    for w in loads[4:11]:
        w.wait()
    sub = lax.broadcasted_iota(jnp.int32, (rows, rows), 0)
    route_t = routes_ref[...].astype(jnp.float32)
    score_t = escore_ref[...]
    scale_t = gscore_ref[...] * score_t / jnp.sum(score_t, axis=0, keepdims=True)
    columns = jnp.where(sub == 0, route_t[0:1, :], 0.0) + jnp.where(sub == 1, route_t[1:2, :], 0.0)
    columns = columns.T
    ra = columns[:, 0:1].astype(jnp.int32)
    rb = columns[:, 1:2].astype(jnp.int32)
    elane = lax.broadcasted_iota(jnp.int32, (rows, 128), 1)
    row_i = lax.broadcasted_iota(jnp.int32, (rows, rows), 0)
    col_i = lax.broadcasted_iota(jnp.int32, (rows, rows), 1)
    strict = jnp.where(col_i < row_i, 1.0, 0.0).astype(jnp.bfloat16)
    is_a = elane == ra
    is_b = elane == rb
    either = (jnp.where(is_a, 1.0, 0.0) + jnp.where(is_b, 1.0, 0.0)).astype(jnp.bfloat16)
    before = dot(strict, either)
    rank_a = jnp.sum(jnp.where(is_a, before, 0.0), axis=1, keepdims=True)
    rank_b = jnp.sum(jnp.where(is_b, before, 0.0), axis=1, keepdims=True)
    group = ra // GROUP_SIZE
    is_g = elane == group
    before_g = dot(strict, jnp.where(is_g, 1.0, 0.0).astype(jnp.bfloat16))
    rank_g = jnp.sum(jnp.where(is_g, before_g, 0.0), axis=1, keepdims=True).astype(jnp.int32)
    code_a = ((ra % GROUP_SIZE) * cap + 1).astype(jnp.float32) + rank_a
    code_b = ((rb % GROUP_SIZE) * cap + 1).astype(jnp.float32) + rank_b
    values = jnp.where(elane == 0, code_a, 0.0) + jnp.where(elane == 1, code_b, 0.0)
    values_t = values.T[0:8, :]
    sub8 = lax.broadcasted_iota(jnp.int32, (8, rows), 0)
    values_t = values_t + jnp.where(sub8 == 2, scale_t[0:1, :], 0.0)
    values_t = values_t + jnp.where(sub8 == 3, scale_t[1:2, :], 0.0)
    slot_lane = lax.broadcasted_iota(jnp.int32, (rows, lanes), 1)
    mine = jnp.where(elane == rank_g, 1.0, 0.0)
    for g in range(groups):
        msend[g] = jnp.dot(
            values_t, jnp.where(group == g, mine, 0.0),
            preferred_element_type=jnp.float32, precision=lax.Precision.HIGHEST,
        )
    mrecv[me_g] = msend[me_g]
    for d in range(1, groups):
        g, dev = far(d)
        remote(msend.at[g], mrecv.at[me_g], msem_s.at[0], msem_r.at[0], dev).start()
    metas = batch(msend.at[apart], mrecv.at[apart], msem_s.at[0], msem_r.at[0])
    gt = jnp.where(slot_lane == group * trow + rank_g, 1.0, 0.0)
    gather[...] = gt.T.astype(jnp.bfloat16)
    gt = gt.astype(jnp.bfloat16)
    for h in range(heads):
        hv = slice(h * VALUE_DIM, (h + 1) * VALUE_DIM)
        gated_out[:, hv] = hgain_ref[...] * silu(og_ref[:, hv].astype(jnp.float32))

    hop2.wait_recv()
    state = jnp.zeros((part, keys), jnp.float32)
    for g in range(groups - 1):
        step = factor_of(grecv[g, part : part + 16, :])
        state = jnp.where(me_g > g, step * state + grecv[g, 0:part, :].astype(jnp.float32), state)
    for j in range(quad):
        epack[j] = (before_decay[j] * state + before_state[j]).astype(jnp.bfloat16)
    mine_v = pl.ds(pl.multiple_of(me_q * part, part), part)
    for d in range(1, quad):
        j, dev = side(d)
        remote(epack.at[j], ent.at[mine_v], ms3.at[0], mr3.at[0], dev).start()
    ent[mine_v, :] = epack[me_q]
    slices = pl.ds(0, (quad - 1) * part)
    hop3 = batch(ent.at[slices], ent.at[slices], ms3.at[0], mr3.at[0])
    hop3.wait_recv()
    sends = [hop1, hop2, hop3, metas]
    entering = ent[...]

    def finish(which):
        at = pl.ds(pl.multiple_of(which * rows, rows), rows)
        for h in range(heads):
            pair = slice(h // 2 * 2 * KEY_DIM, (h // 2 + 1) * 2 * KEY_DIM)
            hv = slice(h * VALUE_DIM, (h + 1) * VALUE_DIM)
            attended = within[at, hv] + lax.dot_general(
                of_head(qlead[at, pair], h), entering[:, pair], nt,
                preferred_element_type=jnp.float32,
            )
            mean = jnp.mean(attended * attended, axis=1, keepdims=True)
            unit = attended * lax.rsqrt(mean + 1e-06)
            mix_ref[at, hv] = (unit * gated_out[at, hv]).astype(jnp.bfloat16)

    other = 1 - me_tp
    finish(other)
    mixcopy = remote(
        mix_ref.at[pl.ds(pl.multiple_of(other * rows, rows), rows)], mixin,
        mixsem.at[0], mixsem.at[1], (me_sp, other),
    )
    mixcopy.start()

    finish(me_tp)

    weights[0].wait()
    own = mix_ref[pl.ds(pl.multiple_of(me_tp * rows, rows), rows), :]
    own_w = pl.multiple_of(me_tp * half, half)
    oth_w = pl.multiple_of(other * half, half)
    cols = [pl.ds(k * chunk, chunk) for k in range(CHUNKS)]
    part = [dot(own, wo[pl.ds(own_w, half), c]) for c in cols]
    mixcopy.wait_recv()
    peer = mixin[...]
    square = jnp.zeros((rows, 1), jnp.float32)
    for k, c in enumerate(cols):
        total = part[k] + dot(peer, wo[pl.ds(oth_w, half), c])
        summed = (res_ref[:, c].astype(jnp.float32) + total).astype(jnp.bfloat16)
        merged[:, c] = summed
        wide = summed.astype(jnp.float32)
        square = square + jnp.sum(wide * wide, axis=1, keepdims=True)
    inv = lax.rsqrt(square / width + 1e-06)
    for c in cols:
        normed[:, c] = (merged[:, c].astype(jnp.float32) * inv * gain_ref[:, c]).astype(
            jnp.bfloat16
        )

    if lanes > groups * trow:
        pad = lanes - groups * trow
        zrecv[pl.ds(groups * trow, pad), :] = jnp.zeros((pad, width), bf)
    far_rows = lambda g: pl.ds(pl.multiple_of(g * trow, 16), trow)
    near_rows = lambda l: pl.ds(pl.multiple_of(l * TILE, TILE), TILE)
    sends.append(mixcopy)
    order = arrival_order(me_g, groups)

    def home(g):
        return (g * quad + me_q, me_tp)

    early = [pl.ds(0, 2 * narrow)] + [pl.ds((t + 1) * narrow, narrow) for t in range(1, packs)]
    late = [pl.ds(t * narrow, narrow) for t in range(packs - 1)]
    late = late + [pl.ds((packs - 1) * narrow, 2 * narrow)]

    def from_far(i, t):
        there = (far_rows(order[i]), early[t])
        return remote(
            sbuf.at[there], rbuf.at[there], s1.at[0], r1.at[order[i], t], home(order[i])
        )

    ready = normed[...]
    for g in send_order(me_g, groups):
        sbuf[far_rows(g), :] = dot(gather[far_rows(g), :], ready).astype(bf)
        for t in range(packs):
            remote(
                sbuf.at[far_rows(g), early[t]], rbuf.at[far_rows(me_g), early[t]],
                s1.at[0], r1.at[me_g, t], home(g),
            ).start()
    rbuf[far_rows(me_g), :] = dot(gather[far_rows(me_g), :], ready).astype(bf)
    metas.wait_recv()
    out_rows = pl.ds(0, (groups - 1) * trow)
    sends.append(batch(sbuf.at[out_rows], sbuf.at[out_rows], s1.at[0], r1.at[0, 0]))

    slab = GROUP_SIZE * TILE
    parts = [pl.ds(t * narrow, narrow) for t in range(packs)]
    taken = [pl.ds((t + 1) * narrow, narrow) for t in range(packs)]
    lead = pl.ds(0, narrow)
    last = pl.ds(bulk, narrow)

    def keys_of(row, t, p):
        at = row % TILE
        slot = at if t is None else packs * (at - slots) + t
        valid = at < slots if t is None else at >= slots
        if per > 1:
            valid = valid & (slot // cap == p)
        return jnp.where(valid, (row // TILE) * cap + slot - p * cap + 1, -1).astype(jnp.float32)

    down_row = lax.broadcasted_iota(jnp.int32, (slab, trow), 0)
    across_row = lax.broadcasted_iota(jnp.int32, (trow, slab), 1)
    sq_i = lax.broadcasted_iota(jnp.int32, (slab, slab), 0)
    sq_j = lax.broadcasted_iota(jnp.int32, (slab, slab), 1)

    def pairs_of(packed, plain, t):
        same = packed // TILE == plain // TILE
        at = packed % TILE
        hit = same & (at >= slots) & (plain % TILE == packs * (at - slots) + t)
        return jnp.where(hit & (plain % TILE < slots), 1.0, 0.0).astype(bf)

    unpack = [pairs_of(sq_j, sq_i, t) for t in range(packs)]
    repack = [pairs_of(sq_i, sq_j, t) for t in range(packs)]
    plain_row = lax.broadcasted_iota(jnp.int32, (slab, narrow), 0) % TILE < slots

    peers = pl.ds(0, (GROUP_SIZE - 1) * TILE)

    def spread(u, t, src, dst, send, recv):
        for d in range(1, GROUP_SIZE):
            l, dev = near(d)
            remote(
                src.at[u, near_rows(l), parts[t]], dst.at[u, near_rows(me_l), parts[t]],
                send, recv, dev,
            ).start()
        dst[u, near_rows(me_l), parts[t]] = src[u, near_rows(me_l), parts[t]]

    def dispatch(u):
        def pick(p, t):
            table = mrecv[order[u * per + p]][:, 0:trow]
            key = keys_of(down_row, t, p)
            hit = (key == table[0:1, :]) | (key == table[1:2, :])
            return jnp.where(hit, 1.0, 0.0).astype(bf)

        plain = [pick(p, None) for p in range(per)]
        for t in range(packs):
            acc = jnp.zeros((slab, narrow), jnp.float32)
            for p in range(per):
                i = u * per + p
                if i > 0:
                    from_far(i, t).wait_recv()
                acc = acc + dot(plain[p], rbuf[far_rows(order[i]), taken[t]])
                acc = acc + dot(pick(p, t), rbuf[far_rows(order[i]), lead])
            xsend[u, :, parts[t]] = acc.astype(bf)
            spread(u, t, xsend, xin, s2.at[u], r2.at[u])

    def dispatched(u):
        sends.append(batch(xsend.at[u, peers], xin.at[u, peers], s2.at[u], r2.at[u]))
        return sends[-1]

    def experts(u, arriving):
        arriving.wait_recv()
        block = xin[u]
        rest = jnp.zeros((slab, narrow), jnp.float32)
        for t in range(packs):
            rest = rest + dot(unpack[t], xin[u, :, parts[t]])
        rest = rest.astype(bf)
        gated = dot(block, wg[narrow:width, :]) + dot(rest, wg[0:narrow, :])
        lifted = dot(block, wu[narrow:width, :]) + dot(rest, wu[0:narrow, :])
        inner = (silu(gated) * lifted).astype(bf)
        ends = dot(inner, wd[:, last]).astype(bf)
        for t in range(packs):
            main = dot(inner, wd[:, parts[t]])
            ysend[u, :, parts[t]] = jnp.where(plain_row, main, dot(repack[t], ends)).astype(bf)

    def give_back(u):
        for t in range(packs):
            spread(u, t, ysend, yrecv, s3.at[u], r3.at[u, t])

    def given_back(u):
        sends.append(batch(ysend.at[u, peers], ysend.at[u, peers], s3.at[u], r3.at[u, 0]))
        return [
            batch(yrecv.at[u, peers, c], yrecv.at[u, peers, c], s3.at[u], r3.at[u, t])
            for t, c in enumerate(parts)
        ]

    def combine(u, arriving):
        def blend(p, t):
            table = mrecv[order[u * per + p]].T[0:trow, :]
            key = keys_of(across_row, t, p)
            both = jnp.where(key == table[:, 0:1], table[:, 2:3], 0.0)
            both = both + jnp.where(key == table[:, 1:2], table[:, 3:4], 0.0)
            high = both.astype(bf)
            return [high, (both - high.astype(jnp.float32)).astype(bf)]

        plain = [blend(p, None) for p in range(per)]
        ends = [jnp.zeros((trow, narrow), jnp.float32) for _ in range(per)]
        for t in range(packs):
            arriving[t].wait_recv()
            for p in range(per):
                i = u * per + p
                mine_z = far_rows(order[i])
                to = zrecv if i == 0 else zsend
                four = dot(jnp.concatenate(plain[p] + blend(p, t), axis=0), yrecv[u, :, parts[t]])
                to[mine_z, parts[t]] = (four[0:trow] + four[trow : 2 * trow]).astype(bf)
                ends[p] = ends[p] + four[2 * trow : 3 * trow] + four[3 * trow : 4 * trow]
                if t == packs - 1:
                    to[mine_z, last] = ends[p].astype(bf)
                if i > 0:
                    remote(
                        zsend.at[mine_z, late[t]], zrecv.at[far_rows(me_g), late[t]],
                        s4.at[0], r4.at[t], home(order[i]),
                    ).start()

    inner = me_g % 2 + me_g // 2 - 2 * (me_g % 2) * (me_g // 2)

    def at_edge(step, u):
        if groups != 4:
            step(u)
        else:
            pl.when(inner == 0)(lambda: step(u))

    def at_inner(step, u):
        if groups == 4:
            pl.when(inner == 1)(lambda: step(u))

    dispatch(0)
    dispatch(1)
    weights[1].wait()
    weights[2].wait()
    weights[3].wait()
    experts(0, dispatched(0))
    at_inner(give_back, 0)
    at_edge(dispatch, 2)
    experts(1, dispatched(1))
    give_back(1)
    at_inner(dispatch, 2)
    dispatch(3)
    experts(2, dispatched(2))
    give_back(2)
    combine(1, given_back(1))
    experts(3, dispatched(3))
    give_back(3)
    at_edge(give_back, 0)
    combine(2, given_back(2))
    combine(3, given_back(3))
    combine(0, given_back(0))
    for t, c in enumerate(late):
        batch(zsend.at[out_rows, c], zrecv.at[out_rows, c], s4.at[0], r4.at[t]).wait_recv()
        out_ref[:, c] = (merged[:, c].astype(jnp.float32) + dot(gt, zrecv[:, c])).astype(bf)
    sends.append(batch(zsend.at[out_rows], zsend.at[out_rows], s4.at[0], r4.at[0]))
    for m in sends:
        m.wait_send()


def by_place(me, rows):
    odd, high = me % 2, me // 2
    ones = [(1 - odd) * (1 - high), odd * (1 - high), (1 - odd) * high, odd * high]
    return [sum(one * row[i] for one, row in zip(ones, rows)) for i in range(len(rows[0]))]


def send_order(me, count):
    if count != 4:
        return [lax.rem(me + d, count) for d in range(1, count)]
    return by_place(me, ((1, 3, 2), (3, 2, 0), (0, 1, 3), (2, 0, 1)))


def arrival_order(me, count):
    if count != 4:
        return [me] + [lax.rem(me + count - d, count) for d in range(1, count)]
    return [me] + by_place(me, ((2, 3, 1), (0, 3, 2), (3, 0, 1), (1, 0, 2)))


def rbuf_rows(rows, sp, tp):
    cap = 3 * rows // (sp * tp)
    most = min(GROUP_SIZE * cap // 2, rows)
    return -(-most // 16) * 16


def layer_call(
    q, k, v, og, gl, head_gain, residual, out_weight, norm_gain, routes, group_score, expert_score, wg, wu, wd
):
    sp, tp = lax.axis_size("sp"), lax.axis_size("tp")
    rows, width = residual.shape
    groups = sp * tp // GROUP_SIZE
    cap = 3 * rows // (sp * tp)
    lanes = -(-groups * rbuf_rows(rows, sp, tp) // 128) * 128
    slab = (UNITS, GROUP_SIZE * TILE, width * (groups // UNITS) * cap // TILE)
    quad = GROUP_SIZE // tp
    part = VALUE_DIM // quad
    keys = q.shape[1]
    vm = pl.BlockSpec(memory_space=pltpu.VMEM)
    hb = pl.BlockSpec(memory_space=pl.ANY)
    bf = jnp.bfloat16
    dma = pltpu.SemaphoreType.DMA
    packs = slab[2] // (width - slab[2])
    inputs = (
        gl, k, v, q, routes.T, group_score[None, :], expert_score.T,
        og, head_gain[None, :], residual, norm_gain[None, :],
    )
    return pl.pallas_call(
        functools.partial(layer_kernel, sp, tp),
        out_shape=pltpu.VMEM((rows, width), bf),
        in_specs=[hb] * 15,
        out_specs=vm,
        scratch_shapes=[
            *[pltpu.VMEM(x.shape, x.dtype) for x in inputs],
            pltpu.VMEM(out_weight.shape, bf),
            pltpu.VMEM(wg.shape, bf),
            pltpu.VMEM(wu.shape, bf),
            pltpu.VMEM(wd.shape, bf),
            pltpu.VMEM((rows, v.shape[1]), bf),
            pltpu.VMEM((rows, width), bf),
            pltpu.VMEM((rows, width), bf),
            pltpu.VMEM((lanes, width), bf),
            pltpu.VMEM((lanes, width), bf),
            pltpu.VMEM(slab, bf),
            pltpu.VMEM(slab, bf),
            pltpu.VMEM(slab, bf),
            pltpu.VMEM(slab, bf),
            pltpu.VMEM((lanes, width), bf),
            pltpu.VMEM((lanes, width), bf),
            pltpu.VMEM((groups, 8, 128), jnp.float32),
            pltpu.VMEM((groups, 8, 128), jnp.float32),
            pltpu.VMEM(v.shape, bf),
            pltpu.VMEM((lanes, rows), bf),
            pltpu.VMEM(v.shape, jnp.float32),
            pltpu.VMEM(q.shape, bf),
            pltpu.VMEM(v.shape, jnp.float32),
            pltpu.VMEM((quad, part + 16, keys), bf),
            pltpu.VMEM((quad, part + 16, keys), bf),
            pltpu.VMEM((part + 16, keys), bf),
            pltpu.VMEM((groups, part + 16, keys), bf),
            pltpu.VMEM((quad, part, keys), bf),
            pltpu.VMEM((VALUE_DIM, keys), bf),
            dma((1,)), dma((1,)), dma((1,)), dma((1,)), dma((1,)), dma((1,)),
            dma((15,)), dma((2,)), dma((1,)), dma((1,)),
            dma((1,)), dma((groups, packs)), dma((UNITS,)), dma((UNITS,)),
            dma((UNITS,)), dma((UNITS, packs)), dma((1,)), dma((packs,)),
        ],
        compiler_params=pltpu.CompilerParams(
            collective_id=0, has_side_effects=True, vmem_limit_bytes=60 * 1024 * 1024
        ),
    )(*inputs, out_weight, wg, wu, wd)


def local(
    residual,
    queries,
    key_rows,
    value_rows,
    out_gate,
    gate_logits,
    head_gain,
    out_weight,
    norm_gain,
    routes,
    group_score,
    expert_score,
    gate_weight,
    up_weight,
    down_weight,
):
    return layer_call(
        queries, key_rows, value_rows, out_gate, gate_logits, head_gain,
        residual, out_weight, norm_gain, routes, group_score, expert_score,
        gate_weight[0], up_weight[0], down_weight[0],
    )


def solution(mesh):
    placed = (
        P(("sp", "tp"), None),
        P("sp", "tp"),
        P("sp", "tp"),
        P("sp", "tp"),
        P("sp", "tp"),
        P("sp", "tp"),
        P(),
        P(),
        P(),
        P(("sp", "tp"), None),
        P(("sp", "tp")),
        P(("sp", "tp"), None),
        P(("sp", "tp"), None, None),
        P(("sp", "tp"), None, None),
        P(("sp", "tp"), None, None),
    )
    return jax.shard_map(
        local, mesh=mesh, in_specs=placed, out_specs=P(("sp", "tp"), None), check_vma=False
    )
```
